32 devices in a mesh: sp: 8 (over z, y), tp: 4 (over x, core).
Axes of the slice: x: 2, y: 2, z: 4, core: 2. Of those that a mesh axis runs over, the one named last changes fastest.
Arguments:
- stream_in: bfloat16 [2048, 4096], P(('sp', 'tp')), may hold values from -6 to 6
- q_first: bfloat16 [2048, 1024], P('sp', 'tp'), may hold values from -110 to 110
- q_second: bfloat16 [2048, 1024], P('sp', 'tp'), may hold values from -110 to 110
- k_first: bfloat16 [2048, 512], P('sp', 'tp'), may hold values from -7 to 7
- k_second: bfloat16 [2048, 512], P('sp', 'tp'), may hold values from -7 to 7
- values: bfloat16 [2048, 1024], P('sp', 'tp'), may hold values from -6 to 6
- head_lambda: float32 [8], P('tp'), may hold values from 0.3 to 0.8
- w_out: bfloat16 [2048, 4096], P('tp'), may hold values from -0.125 to 0.125
- norm_gain: float32 [4096], replicated, may hold values from 0.1 to 1.9
- routes: int32 [2048, 4], P(('sp', 'tp')), may hold values from 0 to 7, all different within a row; in each aligned block of 64 rows (0 to 63, 64 to 127, ...) at most 48 rows name the same one
- route_w: float32 [2048, 4], P(('sp', 'tp')), may hold values from 0.2 to 1
- w_gate: bfloat16 [8, 4096, 128], P('sp'), may hold values from -0.09375 to 0.09375
- w_up: bfloat16 [8, 4096, 128], P('sp'), may hold values from -0.09375 to 0.09375
- w_down: bfloat16 [8, 128, 4096], P('sp'), may hold values from -0.5 to 0.5
- s_gate: bfloat16 [4096, 512], P(None, 'tp'), may hold values from -0.09375 to 0.09375
- s_up: bfloat16 [4096, 512], P(None, 'tp'), may hold values from -0.09375 to 0.09375
- s_down: bfloat16 [512, 4096], P('tp'), may hold values from -0.25 to 0.25
Outputs:
- layer_out: bfloat16 [2048, 4096], P(('sp', 'tp'))
The draws below stay inside these ranges and needn't reach their ends.
Inputs may be any that keep to these rules, and one draw needn't show every extreme that they name: `routes`: each row names 4 different experts. Within the rows of one device (aligned blocks of 64 rows) no expert is named more than 48 times, and in some blocks one expert is named exactly 48 times.
All inputs are finite; a program needn't handle non-finite values.
Results may differ from the reference program's by a relative error of at most 0.017.
Values may be sent and summed in bfloat16 or wider, within the bound.
A program may use at most 128 MiB of HBM per device.

```python
import math
import jax
import jax.numpy as jnp
import numpy as np
from jax import lax

D = 4096
HEAD = 128
HEADS = 8
KV_HEADS = 4
VD = 256
F = 128
SF = 512
TOPK = 4
ROWS = 64
TOKENS = 2048
EXP = 8
CAP = 48
N_SP = 8
N_TP = 4


def key_table(key, which):
    raw = jnp.clip(jax.random.normal(jax.random.fold_in(key, 100 + which), (TOKENS, KV_HEADS * HEAD), jnp.float32), -4.5, 4.5) * 1.3
    return raw


def query_table(key, which):
    raw = jnp.clip(jax.random.normal(jax.random.fold_in(key, 300 + which), (TOKENS, HEADS * HEAD), jnp.float32), -4.5, 4.5) * 1.3
    return raw


def draw_q_first(key, part):
    return query_table(key, 1).astype(jnp.bfloat16)


def draw_q_second(key, part):
    return query_table(key, 2).astype(jnp.bfloat16)


def draw_k_first(key, part):
    return key_table(key, 1).astype(jnp.bfloat16)


def draw_k_second(key, part):
    return key_table(key, 2).astype(jnp.bfloat16)


def level_of(rng, shape, split, smallest, largest):
    factor_of = 1.0
    for axis_at, blocks in split:
        draws = jax.random.uniform(jax.random.fold_in(jax.random.fold_in(rng, 6), axis_at), (blocks,), jnp.float32, smallest / len(split), largest / len(split))
        factor_of = factor_of * jnp.repeat(jnp.exp(draws), shape[axis_at] // blocks).reshape((-1,) + (1,) * (len(shape) - 1 - axis_at))
    return factor_of


def routed_block(own_key, own, number, rows, amount, top, bound, lean):
    ranking = jax.random.permutation(own_key, amount)
    packed, common = shares(amount, rows * top, bound, lean, True), shares(amount, rows * top, bound, lean, False)
    places = jnp.arange(amount)

    def named(tallies, rotation):
        used = int((tallies > 0).sum())
        fixed = max(1, used // 4)
        shifted = fixed + (places - fixed + rotation * (used - fixed)) % max(1, amount - fixed)
        return jnp.zeros((amount,), jnp.int32).at[ranking[jnp.where(places < fixed, places, shifted)]].set(jnp.asarray(tallies, jnp.int32))

    tallies = jnp.where(number % 4 == 0, named(packed, number // 4), named(common, number - number // 4 - 1))
    mixed = jax.random.permutation(jax.random.fold_in(own, 3), amount)
    source_of, sink = mixed[0:amount // 2 * 2:2], mixed[1:amount // 2 * 2:2]
    margin = jnp.minimum(tallies[source_of] - 1, bound - tallies[sink]) // 2
    margin = jnp.where((source_of == ranking[0]) | (sink == ranking[0]) | (tallies[sink] == 0), 0, jnp.maximum(margin, 0))
    shifted = jax.random.randint(jax.random.fold_in(own, 4), (amount // 2,), 0, 1 << 20) % (margin + 1)
    tallies = tallies.at[source_of].add(-shifted).at[sink].add(shifted)
    labels = jnp.searchsorted(jnp.cumsum(tallies), jnp.arange(rows * top), side="right").astype(jnp.int32)
    grid = labels.reshape(top, rows).T
    grid = grid[jax.random.permutation(jax.random.fold_in(own, 1), rows)]
    rotation = jax.random.randint(jax.random.fold_in(own, 2), (rows, 1), 0, top)
    return jnp.take_along_axis(grid, (jnp.arange(top)[None, :] + rotation) % top, axis=1)


def shares(amount, total, limit, skew, full):
    loads = [(1 << 20) // math.isqrt(standing ** skew) + 1 for standing in range(1, amount + 1)]
    largest = limit if full else min(limit, max(-(-total // amount), total * loads[0] // sum(loads)))
    least = 1 if total - largest >= amount - 1 else 0
    holding, spare = [largest] + [least] * (amount - 1), total - largest - least * (amount - 1)
    while spare > 0:
        candidates = [i for i in range(1, amount) if holding[i] < largest] or [i for i in range(1, amount) if holding[i] < limit]
        mass, left = sum([loads[i] for i in candidates]), spare
        for i in candidates:
            addition = min(limit - holding[i], max(1, left * loads[i] // mass), spare)
            holding[i] = holding[i] + addition
            spare = spare - addition
    return np.array(holding)


def normal_values(key, extent, deviation, most, shards=(), held_as=jnp.bfloat16):
    loudness = level_of(key, extent, shards, -0.22, 0.18) if shards else 1.0
    drawn = jax.random.normal(key, extent, jnp.float32) * deviation * loudness
    return jnp.minimum(jnp.maximum(drawn, -most), most).astype(held_as)


def setup_inputs(seed: int = 0) -> dict:
    keys = jax.random.split(jax.random.key(seed), 18)
    stream_in = normal_values(keys[0], (TOKENS, D), 1.0, 6.0, ((0, 32),))
    q_first = draw_q_first(jax.random.fold_in(keys[17], 71), 0)
    q_second = draw_q_second(jax.random.fold_in(keys[17], 71), 0)
    k_first = draw_k_first(jax.random.fold_in(keys[17], 71), 0)
    k_second = draw_k_second(jax.random.fold_in(keys[17], 71), 0)
    values = normal_values(keys[5], (TOKENS, KV_HEADS * VD), 1.0, 6.0, ((0, 8), (1, 4)))
    head_lambda = jnp.clip(0.3 + 0.5 * jax.random.uniform(keys[6], (HEADS,), jnp.float32) ** level_of(keys[6], (HEADS,), ((0, 4),), -0.2, 0.2), 0.3, 0.8)
    w_out = normal_values(keys[7], (HEADS * VD, D), (HEADS * VD) ** -0.5, 0.125, ((0, 4),))
    norm_gain = jnp.clip(1.0 + 0.18 * jax.random.normal(keys[8], (D,), jnp.float32), 0.1, 1.9)
    routes_keys = jax.random.split(jax.random.fold_in(keys[9], 1), TOKENS // ROWS)
    routes_turns = jax.random.permutation(jax.random.fold_in(keys[9], 3), TOKENS // ROWS)
    routes = jax.vmap(lambda own, number: routed_block(jax.random.fold_in(keys[9], 2), own, number, ROWS, EXP, TOPK, CAP, 1))(routes_keys, routes_turns).reshape((TOKENS, TOPK))
    route_w = jnp.clip(0.2 + 0.8 * jax.random.uniform(keys[10], (TOKENS, TOPK), jnp.float32) ** level_of(keys[10], (TOKENS, TOPK), ((0, 32),), -0.2, 0.2), 0.2, 1.0)
    w_gate = normal_values(keys[11], (EXP, D, F), D ** -0.5, 0.09375, ((0, 8),))
    w_up = normal_values(keys[12], (EXP, D, F), D ** -0.5, 0.09375, ((0, 8),))
    w_down = normal_values(keys[13], (EXP, F, D), F ** -0.5, 0.5, ((0, 8),))
    s_gate = normal_values(keys[14], (D, SF), D ** -0.5, 0.09375, ((1, 4),))
    s_up = normal_values(keys[15], (D, SF), D ** -0.5, 0.09375, ((1, 4),))
    s_down = normal_values(keys[16], (SF, D), SF ** -0.5, 0.25, ((0, 4),))
    return {"stream_in": stream_in, "q_first": q_first, "q_second": q_second, "k_first": k_first, "k_second": k_second, "values": values, "head_lambda": head_lambda, "w_out": w_out, "norm_gain": norm_gain, "routes": routes, "route_w": route_w, "w_gate": w_gate, "w_up": w_up, "w_down": w_down, "s_gate": s_gate, "s_up": s_up, "s_down": s_down}


FLOOR = -1e+30

def absorb(state, first_q, second_q, first_k, second_k, value_rows, query_pos, key_pos):
    allowed = key_pos[None, :] <= query_pos[:, None]
    scale = first_q.shape[-1] ** (-0.5)
    result = []
    pairs = ((first_q, first_k), (second_q, second_k))
    for index in range(2):
        query_rows, key_rows = pairs[index]
        peak, total, accum = (state[3 * index], state[3 * index + 1], state[3 * index + 2])
        scores = jnp.dot(query_rows, key_rows.T, preferred_element_type=jnp.float32) * scale
        scores = jnp.where(allowed, scores, FLOOR)
        raised = jnp.maximum(peak, scores.max(-1))
        weights = jnp.where(allowed, jnp.exp(scores - raised[:, None]), 0.0)
        fade = jnp.exp(peak - raised)
        total = total * fade + weights.sum(-1)
        accum = accum * fade[:, None] + jnp.dot(weights.astype(jnp.bfloat16), value_rows, preferred_element_type=jnp.float32)
        result += [raised, total, accum]
    return tuple(result)

def one_head(first_q, second_q, first_k, second_k, value_rows, weight, span, blocks):

    def per_block(block):
        begin = block * span
        query_one = lax.dynamic_slice_in_dim(first_q, begin, span, 0)
        query_two = lax.dynamic_slice_in_dim(second_q, begin, span, 0)
        query_pos = begin + jnp.arange(span, dtype=jnp.int32)
        peaks = jnp.full((span,), FLOOR, jnp.float32)
        sums = jnp.zeros((span,), jnp.float32)
        accums = jnp.zeros((span, VD), jnp.float32)
        start_state = (peaks, sums, accums, peaks, sums, accums)

        def visit(inner, state):
            key_begin = inner * span
            key_one = lax.dynamic_slice_in_dim(first_k, key_begin, span, 0)
            key_two = lax.dynamic_slice_in_dim(second_k, key_begin, span, 0)
            value_part = lax.dynamic_slice_in_dim(value_rows, key_begin, span, 0)
            key_pos = key_begin + jnp.arange(span, dtype=jnp.int32)
            return absorb(state, query_one, query_two, key_one, key_two, value_part, query_pos, key_pos)
        final = lax.fori_loop(jnp.int32(0), block + 1, visit, start_state)
        head_out = final[2] / final[1][:, None] - weight * final[5] / final[4][:, None]
        head_out = head_out * lax.rsqrt(lax.optimization_barrier(jnp.mean(head_out * head_out, axis=-1, keepdims=True)) + 1e-05)
        return head_out.astype(jnp.bfloat16)
    outputs = lax.map(per_block, jnp.arange(blocks, dtype=jnp.int32))
    return outputs.reshape(TOKENS, VD)

def reference(stream_in, q_first, q_second, k_first, k_second, values, head_lambda, w_out, norm_gain, routes, route_w, w_gate, w_up, w_down, s_gate, s_up, s_down):
    group = HEADS // KV_HEADS
    span = math.gcd(TOKENS, 512)
    blocks = TOKENS // span
    parts = []
    for head in range(HEADS):
        key_head = head // group
        parts.append(one_head(q_first[:, head * HEAD:(head + 1) * HEAD], q_second[:, head * HEAD:(head + 1) * HEAD], k_first[:, key_head * HEAD:(key_head + 1) * HEAD], k_second[:, key_head * HEAD:(key_head + 1) * HEAD], values[:, key_head * VD:(key_head + 1) * VD], head_lambda[head], span, blocks))
    attn_rows = jnp.concatenate(parts, axis=1)
    attn = jnp.dot(attn_rows, w_out, preferred_element_type=jnp.float32)
    resid = (stream_in.astype(jnp.float32) + attn).astype(jnp.bfloat16)
    stream = lax.optimization_barrier(resid).astype(jnp.float32)
    normed = (stream * lax.rsqrt(lax.optimization_barrier(jnp.mean(stream * stream, axis=-1, keepdims=True)) + 1e-06) * norm_gain).astype(jnp.bfloat16)
    shared_hidden = (jax.nn.silu(jnp.dot(normed, s_gate, preferred_element_type=jnp.float32)) * jnp.dot(normed, s_up, preferred_element_type=jnp.float32)).astype(jnp.bfloat16)
    shared = jnp.dot(shared_hidden, s_down, preferred_element_type=jnp.float32)
    flat_ids = routes.reshape(-1).astype(jnp.int32)
    count_all = TOKENS * TOPK
    token_of = jnp.arange(count_all, dtype=jnp.int32) // TOPK
    order = jnp.argsort(flat_ids, stable=True).astype(jnp.int32)
    counts = lax.optimization_barrier(jnp.sum((flat_ids[None, :] == jnp.arange(EXP, dtype=jnp.int32)[:, None]).astype(jnp.int32), axis=1)).astype(jnp.int32)
    starts = (jnp.cumsum(counts) - counts).astype(jnp.int32)
    window = N_SP * N_TP * CAP
    padded = jnp.concatenate([order, jnp.zeros((window,), jnp.int32)])
    flat_weights = route_w.reshape(-1)

    def serve(routed, inputs):
        gate_e, up_e, down_e, begin, count = inputs
        picks = lax.dynamic_slice_in_dim(padded, begin, window, 0)
        live = jnp.arange(window, dtype=jnp.int32) < count
        tokens_here = token_of[picks]
        rows_here = normed[tokens_here]
        hidden = (jax.nn.silu(jnp.dot(rows_here, gate_e, preferred_element_type=jnp.float32)) * jnp.dot(rows_here, up_e, preferred_element_type=jnp.float32)).astype(jnp.bfloat16)
        result = jnp.dot(hidden, down_e, preferred_element_type=jnp.float32).astype(jnp.bfloat16)
        scaled = result.astype(jnp.float32) * jnp.where(live, flat_weights[picks], 0.0)[:, None]
        return (routed.at[tokens_here].add(scaled), None)
    routed, _ = lax.scan(serve, jnp.zeros((TOKENS, D), jnp.float32), (w_gate, w_up, w_down, starts, counts))
    return (stream + routed + shared).astype(jnp.bfloat16)
```

```python
import functools
import math

import jax
import jax.numpy as jnp
from jax import lax
from jax.experimental import pallas as pl
from jax.experimental.pallas import tpu as pltpu
from jax.sharding import PartitionSpec as P

HEAD = 128


FLOOR = -1e30


def absorb(state, first_q, second_q, first_k, second_k, value_rows, query_pos, key_pos):
    allowed = key_pos[None, :] <= query_pos[:, None]
    scale = first_q.shape[-1] ** (-0.5)
    result = []
    pairs = ((first_q, first_k), (second_q, second_k))
    for index in range(2):
        query_rows, key_rows = pairs[index]
        peak, total, accum = (state[3 * index], state[3 * index + 1], state[3 * index + 2])
        scores = (
            jnp.einsum("qagd,kad->agqk", query_rows, key_rows, preferred_element_type=jnp.float32)
            * scale
        )
        scores = jnp.where(allowed, scores, FLOOR)
        raised = jnp.maximum(peak, scores.max(-1))
        weights = jnp.where(allowed, jnp.exp(scores - raised[..., None]), 0.0)
        fade = jnp.exp(peak - raised)
        total = total * fade + weights.sum(-1)
        accum = accum * fade[..., None] + jnp.einsum(
            "agqk,kad->agqd",
            weights.astype(jnp.bfloat16),
            value_rows,
            preferred_element_type=jnp.float32,
        )
        result += [raised, total, accum]
    return tuple(result)


def empty_state(kv_local, group, count, value_dim):
    peaks = jnp.full((kv_local, group, count), FLOOR, jnp.float32)
    sums = jnp.zeros((kv_local, group, count), jnp.float32)
    accums = jnp.zeros((kv_local, group, count, value_dim), jnp.float32)
    return (peaks, sums, accums, peaks, sums, accums)


def fold_rows(state, first_q, second_q, query_pos, last_row, pieces, start):
    first_k, second_k, value_rows = pieces
    length = first_k.shape[0]
    kv_local = first_q.shape[1]
    value_dim = value_rows.shape[1] // kv_local
    span = math.gcd(length, 2048)

    def sweep(current):

        def visit(block, inner):
            begin = block * span
            key_one = lax.dynamic_slice_in_dim(first_k, begin, span, 0).reshape(
                span, kv_local, HEAD
            )
            key_two = lax.dynamic_slice_in_dim(second_k, begin, span, 0).reshape(
                span, kv_local, HEAD
            )
            value_part = lax.dynamic_slice_in_dim(value_rows, begin, span, 0).reshape(
                span, kv_local, value_dim
            )
            key_pos = begin + jnp.arange(span, dtype=jnp.int32)
            return absorb(
                inner, first_q, second_q, key_one, key_two, value_part, query_pos, key_pos
            )

        return lax.fori_loop(0, length // span, visit, current)

    def unchanged(current):
        return current

    return lax.cond(start <= last_row, sweep, unchanged, state)


def finish_heads(final, head_lambda):
    kv_local, group, count, value_dim = final[2].shape
    weight = head_lambda.reshape(kv_local, group, 1, 1)
    head_out = final[2] / final[1][..., None] - weight * final[5] / final[4][..., None]
    head_out = head_out * lax.rsqrt(jnp.mean(head_out * head_out, axis=-1, keepdims=True) + 1e-05)
    return (
        head_out.transpose(2, 0, 1, 3)
        .reshape(count, kv_local * group * value_dim)
        .astype(jnp.bfloat16)
    )


def shared_part(normed, s_gate, s_up, s_down):
    piece = lax.all_gather(normed, "tp", axis=0, tiled=True)
    gate_part = jnp.dot(piece, s_gate, preferred_element_type=jnp.float32)
    up_part = jnp.dot(piece, s_up, preferred_element_type=jnp.float32)
    hidden = (jax.nn.silu(gate_part) * up_part).astype(jnp.bfloat16)
    terms = jnp.dot(hidden, s_down, preferred_element_type=jnp.float32)
    return lax.psum_scatter(
        terms.astype(jnp.bfloat16), "tp", scatter_dimension=0, tiled=True
    ).astype(jnp.float32)


def routed_part(normed, routes, route_w, w_gate, w_up, w_down):
    rows, topk = routes.shape
    local_experts = w_gate.shape[0]
    experts = local_experts * lax.axis_size("sp")
    slots = max(2, 3 * rows * topk // (2 * experts))
    flat_ids = routes.reshape(-1)
    hits = (flat_ids[:, None] == jnp.arange(experts, dtype=jnp.int32)[None, :]).astype(jnp.int32)
    slot_of = jnp.sum(jnp.cumsum(hits, axis=0) * hits, axis=1) - 1
    target = flat_ids * slots + slot_of
    placing = jnp.any(
        jnp.arange(experts * slots, dtype=jnp.int32)[:, None, None]
        == target.reshape(rows, topk)[None, :, :],
        axis=-1,
    ).astype(jnp.bfloat16)
    outgoing = (
        jnp.dot(placing, normed, preferred_element_type=jnp.float32)
        .astype(jnp.bfloat16)
        .reshape(experts, slots, normed.shape[1])
    )
    arrived = lax.all_to_all(outgoing, "sp", split_axis=0, concat_axis=0, tiled=True)
    sources = arrived.shape[0] // local_experts
    grouped = arrived.reshape(sources, local_experts, arrived.shape[1], arrived.shape[2])
    gate_part = jnp.einsum("sjcd,jdf->sjcf", grouped, w_gate, preferred_element_type=jnp.float32)
    up_part = jnp.einsum("sjcd,jdf->sjcf", grouped, w_up, preferred_element_type=jnp.float32)
    hidden = (jax.nn.silu(gate_part) * up_part).astype(jnp.bfloat16)
    result = jnp.einsum(
        "sjcf,jfd->sjcd", hidden, w_down, preferred_element_type=jnp.float32
    ).astype(jnp.bfloat16)
    returned = lax.all_to_all(
        result.reshape(arrived.shape), "sp", split_axis=0, concat_axis=0, tiled=True
    )
    picked = (
        returned.reshape(experts * slots, normed.shape[1])[target]
        .reshape(rows, topk, normed.shape[1])
        .astype(jnp.float32)
    )
    return jnp.sum(picked * route_w[..., None], axis=1)


def local(
    stream_in,
    q_first,
    q_second,
    k_first,
    k_second,
    values,
    head_lambda,
    w_out,
    norm_gain,
    routes,
    route_w,
    w_gate,
    w_up,
    w_down,
    s_gate,
    s_up,
    s_down,
):
    seq_rows = q_first.shape[0]
    kv_local = k_first.shape[1] // HEAD
    heads_local = q_first.shape[1] // HEAD
    group = heads_local // kv_local
    value_dim = values.shape[1] // kv_local
    offset = lax.axis_index("sp") * seq_rows
    query_pos = offset + jnp.arange(seq_rows, dtype=jnp.int32)
    last_row = offset + seq_rows - 1
    first_q = q_first.reshape(seq_rows, kv_local, group, HEAD)
    second_q = q_second.reshape(seq_rows, kv_local, group, HEAD)
    start_state = empty_state(kv_local, group, seq_rows, value_dim)
    folded_state = fold_rows(
        start_state,
        first_q,
        second_q,
        query_pos,
        last_row,
        (
            lax.all_gather(k_first, "sp", axis=0, tiled=True),
            lax.all_gather(k_second, "sp", axis=0, tiled=True),
            lax.all_gather(values, "sp", axis=0, tiled=True),
        ),
        jnp.int32(0),
    )
    attn_rows = finish_heads(folded_state, head_lambda)
    attn = lax.psum_scatter(
        jnp.dot(attn_rows, w_out, preferred_element_type=jnp.float32).astype(jnp.bfloat16),
        "tp",
        scatter_dimension=0,
        tiled=True,
    ).astype(jnp.float32)
    resid = (stream_in.astype(jnp.float32) + attn).astype(jnp.bfloat16)
    stream = lax.optimization_barrier(resid).astype(jnp.float32)
    normed = (
        stream * lax.rsqrt(jnp.mean(stream * stream, axis=-1, keepdims=True) + 1e-06) * norm_gain
    ).astype(jnp.bfloat16)
    routed = routed_part(normed, routes, route_w, w_gate, w_up, w_down)
    shared = shared_part(normed, s_gate, s_up, s_down)
    return (stream + routed + shared).astype(jnp.bfloat16)


def mesh_copy(src, dst, send_sem, recv_sem, axis, target):
    return pltpu.make_async_remote_copy(
        src_ref=src,
        dst_ref=dst,
        send_sem=send_sem,
        recv_sem=recv_sem,
        device_id={axis: target},
        device_id_type=pl.DeviceIdType.MESH,
    )


def greet(axis, target):
    pl.semaphore_signal(
        pltpu.get_barrier_semaphore(),
        inc=1,
        device_id={axis: target},
        device_id_type=pl.DeviceIdType.MESH,
    )


def attend_kernel(
    n,
    group,
    q_one,
    q_two,
    k_one,
    k_two,
    val,
    lam,
    out,
    stacked,
    keys_one,
    keys_two,
    vals,
    peak,
    total,
    accum,
    send_sem,
    recv_sem,
):
    me = lax.axis_index("sp")
    place, side = me // 2, me % 2
    depth = n // 2
    pair = me + 1 - 2 * side
    above = place < depth - 1
    rows = q_one.shape[0]
    sources = (k_one, k_two, val)
    held = (keys_one, keys_two, vals)
    scale = HEAD ** (-0.5)

    @pl.when(place > 0)
    def _():
        greet("sp", me - 2)

    @pl.when(above)
    def _():
        greet("sp", me + 2)

    greet("sp", pair)
    pl.semaphore_wait(
        pltpu.get_barrier_semaphore(),
        1 + (place > 0).astype(jnp.int32) + above.astype(jnp.int32),
    )

    def copies(block, way, target, own):
        return [
            mesh_copy(
                sources[a] if own else held[a].at[block],
                held[a].at[block],
                send_sem.at[way, a, block],
                recv_sem.at[a, block],
                "sp",
                target,
            )
            for a in range(3)
        ]

    def start(block, way, target, own=False):
        for one in copies(block, way, target, own):
            one.start()

    def arrive(block):
        for one in copies(block, 0, pair, False):
            one.wait_recv()

    @pl.when(above)
    def _():
        start(me, 0, me + 2, True)

    @pl.when(side == 0)
    def _():
        start(me, 1, pair, True)

    for index, q in enumerate((q_one, q_two)):
        for h in range(group):
            stacked[index, h * rows : (h + 1) * rows, :] = q[:, h * HEAD : (h + 1) * HEAD]

    def scores_of(index, keys):
        return (
            lax.dot_general(
                stacked[index], keys, (((1,), (1,)), ((), ())), preferred_element_type=jnp.float32
            )
            * scale
        )

    spread = (group * rows, rows)
    row_of = lax.broadcasted_iota(jnp.int32, spread, 0) % rows
    allowed = lax.broadcasted_iota(jnp.int32, spread, 1) <= row_of
    for index, keys in enumerate((k_one, k_two)):
        scores = jnp.where(allowed, scores_of(index, keys[...]), FLOOR)
        top = jnp.max(scores, axis=-1, keepdims=True)
        weights = jnp.exp(scores - top)
        peak[index] = top
        total[index] = jnp.sum(weights, axis=-1, keepdims=True)
        accum[index] = jnp.dot(
            weights.astype(jnp.bfloat16), val[...], preferred_element_type=jnp.float32
        )

    def fold(block):
        for index in range(2):
            scores = scores_of(index, held[index][block])
            old = peak[index]
            top = jnp.maximum(old, jnp.max(scores, axis=-1, keepdims=True))
            weights = jnp.exp(scores - top)
            fade = jnp.exp(old - top)
            peak[index] = top
            total[index] = total[index] * fade + jnp.sum(weights, axis=-1, keepdims=True)
            accum[index] = accum[index] * fade + jnp.dot(
                weights.astype(jnp.bfloat16), vals[block], preferred_element_type=jnp.float32
            )

    def visit(e, carry):
        @pl.when(place >= e)
        def _():
            block = me - 2 * e
            arrive(block)

            @pl.when(above)
            def _():
                start(block, 0, me + 2)

            start(block, 1, pair)
            fold(block)

        @pl.when((place >= e - 1) & ((e > 1) | (side == 1)))
        def _():
            block = pair - 2 * (e - 1)
            arrive(block)
            fold(block)

        return carry

    lax.fori_loop(1, depth + 1, visit, 0)

    for h in range(group):
        part = slice(h * rows, (h + 1) * rows)
        head = accum[0, part, :] / total[0, part, :] - lam[h] * (
            accum[1, part, :] / total[1, part, :]
        )
        head = head * lax.rsqrt(jnp.mean(head * head, axis=-1, keepdims=True) + 1e-05)
        width = head.shape[1]
        out[:, h * width : (h + 1) * width] = head.astype(jnp.bfloat16)

    def settle(e, carry):
        @pl.when(place >= e)
        def _():
            block = me - 2 * e

            @pl.when(above)
            def _():
                for one in copies(block, 0, me + 2, False):
                    one.wait_send()

            @pl.when((e > 0) | (side == 0))
            def _():
                for one in copies(block, 1, pair, False):
                    one.wait_send()

        return carry

    lax.fori_loop(0, depth, settle, 0)


def attend(n, q_first, q_second, k_first, k_second, values, head_lambda):
    rows = q_first.shape[0]
    group = q_first.shape[1] // HEAD
    value_dim = values.shape[1]
    vmem = pl.BlockSpec(memory_space=pltpu.VMEM)
    tall = group * rows
    flops = 4 * tall * n * rows * (HEAD + value_dim)
    return pl.pallas_call(
        functools.partial(attend_kernel, n, group),
        out_shape=jax.ShapeDtypeStruct((rows, group * value_dim), jnp.bfloat16),
        in_specs=[vmem] * 5 + [pl.BlockSpec(memory_space=pltpu.SMEM)],
        out_specs=vmem,
        scratch_shapes=[
            pltpu.VMEM((2, tall, HEAD), jnp.bfloat16),
            pltpu.VMEM((n, rows, HEAD), jnp.bfloat16),
            pltpu.VMEM((n, rows, HEAD), jnp.bfloat16),
            pltpu.VMEM((n, rows, value_dim), jnp.bfloat16),
            pltpu.VMEM((2, tall, 1), jnp.float32),
            pltpu.VMEM((2, tall, 1), jnp.float32),
            pltpu.VMEM((2, tall, value_dim), jnp.float32),
            pltpu.SemaphoreType.DMA((2, 3, n)),
            pltpu.SemaphoreType.DMA((3, n)),
        ],
        compiler_params=pltpu.CompilerParams(collective_id=0, has_side_effects=True),
        cost_estimate=pl.CostEstimate(flops=flops * 8, bytes_accessed=1 << 24, transcendentals=0),
        name="attend",
    )(q_first, q_second, k_first, k_second, values, head_lambda)


def project_kernel(
    nt, pieces, rows_in, w, stream, gain, resid, normed, order, out_one, in_one, out_two, in_two,
    send_one, recv_one, send_two, recv_two,
):
    me = lax.axis_index("tp")
    far, near = me // 2, me % 2
    partner = me + 1 - 2 * near
    half = nt // 2
    rows = stream.shape[0]
    wide = w.shape[1] // pieces
    greet("tp", partner)
    for o in range(1, half):
        greet("tp", 2 * ((far + o) % half) + near)
    pl.semaphore_wait(pltpu.get_barrier_semaphore(), half)

    for o in range(half):
        base = 2 * ((far + o) % half)
        for which, parity in enumerate((1 - near, near)):
            begin = pl.multiple_of((base + parity) * rows, rows)
            order[which, o * rows : (o + 1) * rows, :] = rows_in[pl.ds(begin, rows), :]

    first = [
        mesh_copy(out_one.at[i], in_one.at[i], send_one.at[i], recv_one.at[i], "tp", partner)
        for i in range(pieces)
    ]
    second = [
        [
            mesh_copy(
                out_two.at[o, i],
                in_two.at[o, i],
                send_two.at[o, i],
                recv_two.at[o, i],
                "tp",
                2 * ((far + o + 1) % half) + near,
            )
            for o in range(half - 1)
        ]
        for i in range(pieces)
    ]
    for i in range(pieces):
        column = slice(i * wide, (i + 1) * wide)
        out_one[i] = jnp.dot(
            order[0], w[:, column], preferred_element_type=jnp.float32
        ).astype(jnp.bfloat16)
        first[i].start()
    kept = []
    for i in range(pieces):
        column = slice(i * wide, (i + 1) * wide)
        part = jnp.dot(order[1], w[:, column], preferred_element_type=jnp.float32)
        first[i].wait_recv()
        part = part + in_one[i].astype(jnp.float32)
        for o in range(half - 1):
            out_two[o, i] = part[(o + 1) * rows : (o + 2) * rows].astype(jnp.bfloat16)
            second[i][o].start()
        kept.append(part[:rows])
    squares = jnp.zeros((rows, 1), jnp.float32)
    for i in range(pieces):
        column = slice(i * wide, (i + 1) * wide)
        part = kept[i]
        for o in range(half - 1):
            second[i][o].wait_recv()
            part = part + in_two[o, i].astype(jnp.float32)
        sums = (stream[:, column].astype(jnp.float32) + part).astype(jnp.bfloat16)
        resid[:, column] = sums
        sums = sums.astype(jnp.float32)
        squares = squares + jnp.sum(sums * sums, axis=-1, keepdims=True)
    shrink = lax.rsqrt(squares / stream.shape[1] + 1e-06)
    for i in range(pieces):
        column = slice(i * wide, (i + 1) * wide)
        normed[:, column] = (
            resid[:, column].astype(jnp.float32) * shrink * gain[:, column]
        ).astype(jnp.bfloat16)
    for i in range(pieces):
        first[i].wait_send()
        for o in range(half - 1):
            second[i][o].wait_send()


def project(nt, attn_rows, w_out, stream_in, norm_gain):
    rows, width = stream_in.shape
    pieces = 4
    wide = width // pieces
    half = nt // 2
    vmem = pl.BlockSpec(memory_space=pltpu.VMEM)
    shape = jax.ShapeDtypeStruct((rows, width), jnp.bfloat16)
    flops = 2 * attn_rows.shape[0] * attn_rows.shape[1] * width
    return pl.pallas_call(
        functools.partial(project_kernel, nt, pieces),
        out_shape=(shape, shape),
        in_specs=[vmem] * 4,
        out_specs=(vmem, vmem),
        scratch_shapes=[
            pltpu.VMEM((2, half * rows, attn_rows.shape[1]), jnp.bfloat16),
            pltpu.VMEM((pieces, half * rows, wide), jnp.bfloat16),
            pltpu.VMEM((pieces, half * rows, wide), jnp.bfloat16),
            pltpu.VMEM((half - 1, pieces, rows, wide), jnp.bfloat16),
            pltpu.VMEM((half - 1, pieces, rows, wide), jnp.bfloat16),
            pltpu.SemaphoreType.DMA((pieces,)),
            pltpu.SemaphoreType.DMA((pieces,)),
            pltpu.SemaphoreType.DMA((half - 1, pieces)),
            pltpu.SemaphoreType.DMA((half - 1, pieces)),
        ],
        compiler_params=pltpu.CompilerParams(collective_id=1, has_side_effects=True),
        cost_estimate=pl.CostEstimate(flops=flops * 8, bytes_accessed=1 << 24, transcendentals=0),
        name="project",
    )(attn_rows, w_out, stream_in, norm_gain.reshape(1, width))


def hidden_kernel(
    n, nt, x, gate, up, s_gate, s_up, mix, out, gathered, beside, out_hid, in_hid, out_sh, in_sh,
    send_x, recv_x, send_b, recv_b, send_h, recv_h, send_s, recv_s,
):
    me, mine = lax.axis_index("sp"), lax.axis_index("tp")
    place, side = me // 2, me % 2
    depth = n // 2
    pair = me + 1 - 2 * side
    above, below = place < depth - 1, place > 0
    hid = gate.shape[1]
    for o in range(1, n):
        greet("sp", (me + o) % n)
    for o in range(1, nt):
        greet("tp", (mine + o) % nt)
    pl.semaphore_wait(pltpu.get_barrier_semaphore(), n + nt - 2)

    def row_copy(block, way, target, own=False):
        return mesh_copy(
            x if own else gathered.at[block],
            gathered.at[block],
            send_x.at[way, block],
            recv_x.at[block],
            "sp",
            target,
        )

    def hid_copy(block):
        return mesh_copy(
            out_hid.at[block], in_hid.at[me], send_h.at[block], recv_h.at[me], "sp", block
        )

    def hid_arrival(block):
        return mesh_copy(
            out_hid.at[block], in_hid.at[block], send_h.at[block], recv_h.at[block], "sp", block
        )

    @pl.when(above)
    def _():
        row_copy(me, 0, me + 2, True).start()

    @pl.when(below)
    def _():
        row_copy(me, 1, me - 2, True).start()

    row_copy(me, 2, pair, True).start()
    side_copies = [
        mesh_copy(
            x, beside.at[o - 1], send_b.at[o - 1], recv_b.at[o - 1], "tp", (mine + o) % nt
        )
        for o in range(1, nt)
    ]
    for one in side_copies:
        one.start()

    def hidden_of(block_rows, g, u):
        gate_part = jnp.dot(block_rows, g[...], preferred_element_type=jnp.float32)
        up_part = jnp.dot(block_rows, u[...], preferred_element_type=jnp.float32)
        return (gate_part / (1.0 + jnp.exp(-gate_part)) * up_part).astype(jnp.bfloat16)

    in_hid[me] = hidden_of(x[...], gate, up)
    in_sh[mine] = hidden_of(x[...], s_gate, s_up)

    def serve(block):
        out_hid[block] = hidden_of(gathered[block], gate, up)
        hid_copy(block).start()

    shared_copies = [
        mesh_copy(
            out_sh.at[o - 1],
            in_sh.at[mine],
            send_s.at[o - 1],
            recv_s.at[mine],
            "tp",
            (mine + nt - o) % nt,
        )
        for o in range(1, nt)
    ]

    def visit(e, carry):
        low, high = place >= e, place + e < depth

        @pl.when(low)
        def _():
            block = me - 2 * e
            row_copy(block, 0, pair).wait_recv()

            @pl.when(above)
            def _():
                row_copy(block, 0, me + 2).start()

            row_copy(block, 2, pair).start()

        @pl.when(high)
        def _():
            block = me + 2 * e
            row_copy(block, 0, pair).wait_recv()

            @pl.when(below)
            def _():
                row_copy(block, 1, me - 2).start()

            row_copy(block, 2, pair).start()

        @pl.when(low)
        def _():
            serve(me - 2 * e)

        @pl.when(high)
        def _():
            serve(me + 2 * e)

        @pl.when(place >= e - 1)
        def _():
            block = pair - 2 * (e - 1)
            row_copy(block, 0, pair).wait_recv()
            serve(block)

        @pl.when((e > 1) & (place + e - 1 < depth))
        def _():
            block = pair + 2 * (e - 1)
            row_copy(block, 0, pair).wait_recv()
            serve(block)

        @pl.when(e == depth - 1)
        def _():
            for o in range(1, nt):
                side_copies[o - 1].wait_recv()
                out_sh[o - 1] = hidden_of(beside[o - 1], s_gate, s_up)
                shared_copies[o - 1].start()

        return carry

    lax.fori_loop(1, depth + 1, visit, 0)

    for o in range(1, n):
        hid_arrival((me + o) % n).wait_recv()
    for o in range(1, nt):
        source = (mine + o) % nt
        mesh_copy(
            out_sh.at[o - 1], in_sh.at[source], send_s.at[o - 1], recv_s.at[source], "tp", source
        ).wait_recv()
    for j in range(n):
        out[:, j * hid : (j + 1) * hid] = (
            in_hid[j].astype(jnp.float32) * mix[:, j : j + 1]
        ).astype(jnp.bfloat16)
    wide = s_gate.shape[1]
    for j in range(nt):
        out[:, n * hid + j * wide : n * hid + (j + 1) * wide] = in_sh[j]

    def settle(block, carry):
        spot = block // 2

        @pl.when(block % 2 == side)
        def _():
            row_copy(block, 2, pair).wait_send()

            @pl.when(above & (spot <= place))
            def _():
                row_copy(block, 0, me + 2).wait_send()

            @pl.when(below & (spot >= place))
            def _():
                row_copy(block, 1, me - 2).wait_send()

        @pl.when(block != me)
        def _():
            hid_copy(block).wait_send()

        return carry

    lax.fori_loop(0, n, settle, 0)
    for o in range(1, nt):
        side_copies[o - 1].wait_send()
        shared_copies[o - 1].wait_send()


def hidden_units(n, nt, normed, w_gate, w_up, s_gate, s_up, mix):
    rows, width = normed.shape
    hid, wide = w_gate.shape[1], s_gate.shape[1]
    vmem = pl.BlockSpec(memory_space=pltpu.VMEM)
    flops = 4 * rows * width * (n * hid + nt * wide)
    return pl.pallas_call(
        functools.partial(hidden_kernel, n, nt),
        out_shape=jax.ShapeDtypeStruct((rows, n * hid + nt * wide), jnp.bfloat16),
        in_specs=[vmem] * 6,
        out_specs=vmem,
        scratch_shapes=[
            pltpu.VMEM((n, rows, width), jnp.bfloat16),
            pltpu.VMEM((nt - 1, rows, width), jnp.bfloat16),
            pltpu.VMEM((n, rows, hid), jnp.bfloat16),
            pltpu.VMEM((n, rows, hid), jnp.bfloat16),
            pltpu.VMEM((nt - 1, rows, wide), jnp.bfloat16),
            pltpu.VMEM((nt, rows, wide), jnp.bfloat16),
            pltpu.SemaphoreType.DMA((3, n)),
            pltpu.SemaphoreType.DMA((n,)),
            pltpu.SemaphoreType.DMA((nt - 1,)),
            pltpu.SemaphoreType.DMA((nt - 1,)),
            pltpu.SemaphoreType.DMA((n,)),
            pltpu.SemaphoreType.DMA((n,)),
            pltpu.SemaphoreType.DMA((nt - 1,)),
            pltpu.SemaphoreType.DMA((nt,)),
        ],
        compiler_params=pltpu.CompilerParams(collective_id=2, has_side_effects=True),
        cost_estimate=pl.CostEstimate(flops=flops * 40, bytes_accessed=1 << 24, transcendentals=0),
        name="hidden_units",
    )(normed, w_gate, w_up, s_gate, s_up, mix)


def near(
    stream_in,
    q_first,
    q_second,
    k_first,
    k_second,
    values,
    head_lambda,
    w_out,
    norm_gain,
    routes,
    route_w,
    w_gate,
    w_up,
    w_down,
    s_gate,
    s_up,
    s_down,
):
    n, nt = lax.axis_size("sp"), lax.axis_size("tp")
    hid, wide = w_down.shape[1], s_down.shape[0]
    routed_piece = lax.dynamic_slice_in_dim(
        w_down[0], lax.axis_index("tp") * (hid // nt), hid // nt, 0
    )
    shared_piece = lax.dynamic_slice_in_dim(
        s_down, lax.axis_index("sp") * (wide // n), wide // n, 0
    )
    routed_down = lax.all_gather(routed_piece, ("sp", "tp"), axis=0, tiled=True)
    shared_down = lax.all_gather(shared_piece, ("tp", "sp"), axis=0, tiled=True)
    attn_rows = attend(n, q_first, q_second, k_first, k_second, values, head_lambda)
    resid, normed = project(nt, attn_rows, w_out, stream_in, norm_gain)
    chosen = routes[:, :, None] == jnp.arange(n, dtype=jnp.int32)[None, None, :]
    mix = jnp.sum(jnp.where(chosen, route_w[:, :, None], 0.0), axis=1)
    units = hidden_units(n, nt, normed, w_gate[0], w_up[0], s_gate, s_up, mix)
    routed = jnp.dot(units[:, : n * hid], routed_down, preferred_element_type=jnp.float32)
    shared = jnp.dot(units[:, n * hid :], shared_down, preferred_element_type=jnp.float32)
    return (resid.astype(jnp.float32) + routed + shared).astype(jnp.bfloat16)


def layer(*arrays):
    n, nt = lax.axis_size("sp"), lax.axis_size("tp")
    k_first, values, w_gate, w_down, s_down = (arrays[i] for i in (3, 5, 11, 13, 16))
    fits = (
        2 <= n <= 16
        and n % 2 == 0
        and nt >= 4
        and nt % 2 == 0
        and k_first.shape[1] == HEAD
        and w_gate.shape[0] == 1
        and w_down.shape[1] % (16 * nt) == 0
        and s_down.shape[0] % (16 * n) == 0
    )
    return near(*arrays) if fits else local(*arrays)


def solution(mesh):
    return jax.shard_map(
        layer,
        mesh=mesh,
        in_specs=(
            P(("sp", "tp"), None),
            P("sp", "tp"),
            P("sp", "tp"),
            P("sp", "tp"),
            P("sp", "tp"),
            P("sp", "tp"),
            P("tp"),
            P("tp", None),
            P(),
            P(("sp", "tp"), None),
            P(("sp", "tp"), None),
            P("sp", None, None),
            P("sp", None, None),
            P("sp", None, None),
            P(None, "tp"),
            P(None, "tp"),
            P("tp", None),
        ),
        out_specs=P(("sp", "tp"), None),
        check_vma=False,
    )
```

```python
import functools
import math

import jax
import jax.numpy as jnp
from jax import lax
from jax.experimental import pallas as pl
from jax.experimental.pallas import tpu as pltpu
from jax.sharding import PartitionSpec as P

HEAD = 128


FLOOR = -1e30


def absorb(state, first_q, second_q, first_k, second_k, value_rows, query_pos, key_pos):
    allowed = key_pos[None, :] <= query_pos[:, None]
    scale = first_q.shape[-1] ** (-0.5)
    result = []
    pairs = ((first_q, first_k), (second_q, second_k))
    for index in range(2):
        query_rows, key_rows = pairs[index]
        peak, total, accum = (state[3 * index], state[3 * index + 1], state[3 * index + 2])
        scores = (
            jnp.einsum("qagd,kad->agqk", query_rows, key_rows, preferred_element_type=jnp.float32)
            * scale
        )
        scores = jnp.where(allowed, scores, FLOOR)
        raised = jnp.maximum(peak, scores.max(-1))
        weights = jnp.where(allowed, jnp.exp(scores - raised[..., None]), 0.0)
        fade = jnp.exp(peak - raised)
        total = total * fade + weights.sum(-1)
        accum = accum * fade[..., None] + jnp.einsum(
            "agqk,kad->agqd",
            weights.astype(jnp.bfloat16),
            value_rows,
            preferred_element_type=jnp.float32,
        )
        result += [raised, total, accum]
    return tuple(result)


def empty_state(kv_local, group, count, value_dim):
    peaks = jnp.full((kv_local, group, count), FLOOR, jnp.float32)
    sums = jnp.zeros((kv_local, group, count), jnp.float32)
    accums = jnp.zeros((kv_local, group, count, value_dim), jnp.float32)
    return (peaks, sums, accums, peaks, sums, accums)


def fold_rows(state, first_q, second_q, query_pos, last_row, pieces, start):
    first_k, second_k, value_rows = pieces
    length = first_k.shape[0]
    kv_local = first_q.shape[1]
    value_dim = value_rows.shape[1] // kv_local
    span = math.gcd(length, 2048)

    def sweep(current):

        def visit(block, inner):
            begin = block * span
            key_one = lax.dynamic_slice_in_dim(first_k, begin, span, 0).reshape(
                span, kv_local, HEAD
            )
            key_two = lax.dynamic_slice_in_dim(second_k, begin, span, 0).reshape(
                span, kv_local, HEAD
            )
            value_part = lax.dynamic_slice_in_dim(value_rows, begin, span, 0).reshape(
                span, kv_local, value_dim
            )
            key_pos = begin + jnp.arange(span, dtype=jnp.int32)
            return absorb(
                inner, first_q, second_q, key_one, key_two, value_part, query_pos, key_pos
            )

        return lax.fori_loop(0, length // span, visit, current)

    def unchanged(current):
        return current

    return lax.cond(start <= last_row, sweep, unchanged, state)


def finish_heads(final, head_lambda):
    kv_local, group, count, value_dim = final[2].shape
    weight = head_lambda.reshape(kv_local, group, 1, 1)
    head_out = final[2] / final[1][..., None] - weight * final[5] / final[4][..., None]
    head_out = head_out * lax.rsqrt(jnp.mean(head_out * head_out, axis=-1, keepdims=True) + 1e-05)
    return (
        head_out.transpose(2, 0, 1, 3)
        .reshape(count, kv_local * group * value_dim)
        .astype(jnp.bfloat16)
    )


def shared_part(normed, s_gate, s_up, s_down):
    piece = lax.all_gather(normed, "tp", axis=0, tiled=True)
    gate_part = jnp.dot(piece, s_gate, preferred_element_type=jnp.float32)
    up_part = jnp.dot(piece, s_up, preferred_element_type=jnp.float32)
    hidden = (jax.nn.silu(gate_part) * up_part).astype(jnp.bfloat16)
    terms = jnp.dot(hidden, s_down, preferred_element_type=jnp.float32)
    return lax.psum_scatter(
        terms.astype(jnp.bfloat16), "tp", scatter_dimension=0, tiled=True
    ).astype(jnp.float32)


def routed_part(normed, routes, route_w, w_gate, w_up, w_down):
    rows, topk = routes.shape
    local_experts = w_gate.shape[0]
    experts = local_experts * lax.axis_size("sp")
    slots = max(2, 3 * rows * topk // (2 * experts))
    flat_ids = routes.reshape(-1)
    hits = (flat_ids[:, None] == jnp.arange(experts, dtype=jnp.int32)[None, :]).astype(jnp.int32)
    slot_of = jnp.sum(jnp.cumsum(hits, axis=0) * hits, axis=1) - 1
    target = flat_ids * slots + slot_of
    placing = jnp.any(
        jnp.arange(experts * slots, dtype=jnp.int32)[:, None, None]
        == target.reshape(rows, topk)[None, :, :],
        axis=-1,
    ).astype(jnp.bfloat16)
    outgoing = (
        jnp.dot(placing, normed, preferred_element_type=jnp.float32)
        .astype(jnp.bfloat16)
        .reshape(experts, slots, normed.shape[1])
    )
    arrived = lax.all_to_all(outgoing, "sp", split_axis=0, concat_axis=0, tiled=True)
    sources = arrived.shape[0] // local_experts
    grouped = arrived.reshape(sources, local_experts, arrived.shape[1], arrived.shape[2])
    gate_part = jnp.einsum("sjcd,jdf->sjcf", grouped, w_gate, preferred_element_type=jnp.float32)
    up_part = jnp.einsum("sjcd,jdf->sjcf", grouped, w_up, preferred_element_type=jnp.float32)
    hidden = (jax.nn.silu(gate_part) * up_part).astype(jnp.bfloat16)
    result = jnp.einsum(
        "sjcf,jfd->sjcd", hidden, w_down, preferred_element_type=jnp.float32
    ).astype(jnp.bfloat16)
    returned = lax.all_to_all(
        result.reshape(arrived.shape), "sp", split_axis=0, concat_axis=0, tiled=True
    )
    picked = (
        returned.reshape(experts * slots, normed.shape[1])[target]
        .reshape(rows, topk, normed.shape[1])
        .astype(jnp.float32)
    )
    return jnp.sum(picked * route_w[..., None], axis=1)


def local(
    stream_in,
    q_first,
    q_second,
    k_first,
    k_second,
    values,
    head_lambda,
    w_out,
    norm_gain,
    routes,
    route_w,
    w_gate,
    w_up,
    w_down,
    s_gate,
    s_up,
    s_down,
):
    seq_rows = q_first.shape[0]
    kv_local = k_first.shape[1] // HEAD
    heads_local = q_first.shape[1] // HEAD
    group = heads_local // kv_local
    value_dim = values.shape[1] // kv_local
    offset = lax.axis_index("sp") * seq_rows
    query_pos = offset + jnp.arange(seq_rows, dtype=jnp.int32)
    last_row = offset + seq_rows - 1
    first_q = q_first.reshape(seq_rows, kv_local, group, HEAD)
    second_q = q_second.reshape(seq_rows, kv_local, group, HEAD)
    start_state = empty_state(kv_local, group, seq_rows, value_dim)
    folded_state = fold_rows(
        start_state,
        first_q,
        second_q,
        query_pos,
        last_row,
        (
            lax.all_gather(k_first, "sp", axis=0, tiled=True),
            lax.all_gather(k_second, "sp", axis=0, tiled=True),
            lax.all_gather(values, "sp", axis=0, tiled=True),
        ),
        jnp.int32(0),
    )
    attn_rows = finish_heads(folded_state, head_lambda)
    attn = lax.psum_scatter(
        jnp.dot(attn_rows, w_out, preferred_element_type=jnp.float32).astype(jnp.bfloat16),
        "tp",
        scatter_dimension=0,
        tiled=True,
    ).astype(jnp.float32)
    resid = (stream_in.astype(jnp.float32) + attn).astype(jnp.bfloat16)
    stream = lax.optimization_barrier(resid).astype(jnp.float32)
    normed = (
        stream * lax.rsqrt(jnp.mean(stream * stream, axis=-1, keepdims=True) + 1e-06) * norm_gain
    ).astype(jnp.bfloat16)
    routed = routed_part(normed, routes, route_w, w_gate, w_up, w_down)
    shared = shared_part(normed, s_gate, s_up, s_down)
    return (stream + routed + shared).astype(jnp.bfloat16)


def mesh_copy(src, dst, send_sem, recv_sem, axis, target):
    return pltpu.make_async_remote_copy(
        src_ref=src,
        dst_ref=dst,
        send_sem=send_sem,
        recv_sem=recv_sem,
        device_id={axis: target},
        device_id_type=pl.DeviceIdType.MESH,
    )


def greet(axis, target):
    pl.semaphore_signal(
        pltpu.get_barrier_semaphore(),
        inc=1,
        device_id={axis: target},
        device_id_type=pl.DeviceIdType.MESH,
    )


def near_kernel(
    n, nt, group, pieces,
    q_one, q_two, k_one, k_two, val, lam, w_out_h, stream, gain, mix,
    gate_h, up_h, s_gate_h, s_up_h, down_h, s_down_h,
    out,
    stacked, keys_one, keys_two, vals, peak, total, accum, rows_in,
    w, order, out_one, in_one, out_two, in_two, resid,
    gates, ups, s_gate, s_up, wall, gathered, beside, out_hid, in_hid, out_sh, in_sh, units,
    load, send_kv, recv_kv, send_one, recv_one, send_two, recv_two,
    send_g, recv_g, send_d, recv_d, send_sd, recv_sd,
    send_x, recv_x, send_b, recv_b, send_h, recv_h, send_s, recv_s,
):
    me, mine = lax.axis_index("sp"), lax.axis_index("tp")
    place, side = me // 2, me % 2
    far, core = mine // 2, mine % 2
    depth, half = n // 2, nt // 2
    pair, partner = me + 1 - 2 * side, mine + 1 - 2 * core
    above, below = place < depth - 1, place > 0
    seq = q_one.shape[0]
    rows, width = stream.shape
    hid, wide = down_h.shape[0], s_down_h.shape[0]
    scale = HEAD ** (-0.5)

    def fars(o):
        return 2 * ((far + o) % half) + core

    def column(o):
        return 2 * ((place + o) % depth) + side

    loads = [
        pltpu.make_async_copy(source, target, load.at[i])
        for i, (source, target) in enumerate(
            (
                (w_out_h, w),
                (gate_h, gates.at[0]),
                (up_h, ups.at[0]),
                (s_gate_h, s_gate),
                (s_up_h, s_up),
                (down_h, wall.at[pl.ds(pl.multiple_of(me * hid, hid), hid)]),
                (s_down_h, wall.at[pl.ds(pl.multiple_of(n * hid + mine * wide, wide), wide)]),
            )
        )
    ]
    for o in range(1, depth):
        greet("sp", column(o))
    greet("sp", pair)
    for o in range(1, half):
        greet("tp", fars(o))
    greet("tp", partner)
    pl.semaphore_wait(pltpu.get_barrier_semaphore(), depth + half)

    sources = (k_one, k_two, val)
    held = (keys_one, keys_two, vals)

    def copies(block, way, target, own):
        return [
            mesh_copy(
                sources[a] if own else held[a].at[block],
                held[a].at[block],
                send_kv.at[way, a, block],
                recv_kv.at[a, block],
                "sp",
                target,
            )
            for a in range(3)
        ]

    def start(block, way, target, own=False):
        for one in copies(block, way, target, own):
            one.start()

    def arrive(block):
        for one in copies(block, 0, pair, False):
            one.wait_recv()

    share = width // 2
    share_at = pl.ds(pl.multiple_of(core * share, share), share)
    other_at = pl.ds(pl.multiple_of((1 - core) * share, share), share)

    def pair_weights():
        return [
            mesh_copy(
                h.at[share_at], v.at[1, share_at], send_g.at[0, i], recv_g.at[0, i], "sp", pair
            )
            for i, (h, v) in enumerate(((gate_h, gates), (up_h, ups)))
        ]

    def pair_weights_on(at):
        return [
            mesh_copy(
                v.at[1, at], v.at[1, at], send_g.at[1, i], recv_g.at[1, i], "tp", partner
            )
            for i, v in enumerate((gates, ups))
        ]

    part = hid // 2

    def down_at(block, c):
        return wall.at[pl.ds(pl.multiple_of(block * hid + c * part, part), part)]

    def down_own(way, target, axis="sp"):
        return mesh_copy(
            down_h.at[pl.ds(pl.multiple_of(core * part, part), part)],
            down_at(me, core),
            send_d.at[way],
            recv_d.at[0, me],
            axis,
            target,
        )

    def down_pair(block):
        return mesh_copy(
            down_at(block, core),
            down_at(block, core),
            send_d.at[depth + block],
            recv_d.at[0, block],
            "sp",
            pair,
        )

    def down_core(block, c):
        return mesh_copy(
            down_at(block, c),
            down_at(block, c),
            send_d.at[depth + n + block],
            recv_d.at[1, block],
            "tp",
            partner,
        )

    def sd_at(u):
        return wall.at[pl.ds(pl.multiple_of(n * hid + u * wide, wide), wide)]

    def sd_own(way, target):
        return mesh_copy(s_down_h, sd_at(mine), send_sd.at[way], recv_sd.at[mine], "tp", target)

    def sd_on(o, u):
        return mesh_copy(
            sd_at(u), sd_at(u), send_sd.at[half + o - 1], recv_sd.at[u], "tp", partner
        )

    @pl.when(above)
    def _():
        start(me, 0, me + 2, True)

    @pl.when(side == 0)
    def _():
        start(me, 1, pair, True)

    for one in loads:
        one.start()
    for o in range(1, half):
        sd_own(o, fars(o)).start()
    sd_own(0, partner).start()
    for o in range(1, depth):

        @pl.when(place + o >= depth)
        def _():
            down_own(o, column(o)).start()

    for index, q in enumerate((q_one, q_two)):
        for h in range(group):
            stacked[index, h * seq : (h + 1) * seq, :] = q[:, h * HEAD : (h + 1) * HEAD]

    def scores_of(index, keys):
        return (
            lax.dot_general(
                stacked[index], keys, (((1,), (1,)), ((), ())), preferred_element_type=jnp.float32
            )
            * scale
        )

    spread = (group * seq, seq)
    row_of = lax.broadcasted_iota(jnp.int32, spread, 0) % seq
    allowed = lax.broadcasted_iota(jnp.int32, spread, 1) <= row_of
    for index, keys in enumerate((k_one, k_two)):
        scores = jnp.where(allowed, scores_of(index, keys[...]), FLOOR)
        top = jnp.max(scores, axis=-1, keepdims=True)
        weights = jnp.exp(scores - top)
        peak[index] = top
        total[index] = jnp.sum(weights, axis=-1, keepdims=True)
        accum[index] = jnp.dot(
            weights.astype(jnp.bfloat16), val[...], preferred_element_type=jnp.float32
        )

    def fold(block):
        for index in range(2):
            scores = scores_of(index, held[index][block])
            old = peak[index]
            top = jnp.maximum(old, jnp.max(scores, axis=-1, keepdims=True))
            weights = jnp.exp(scores - top)
            fade = jnp.exp(old - top)
            peak[index] = top
            total[index] = total[index] * fade + jnp.sum(weights, axis=-1, keepdims=True)
            accum[index] = accum[index] * fade + jnp.dot(
                weights.astype(jnp.bfloat16), vals[block], preferred_element_type=jnp.float32
            )

    def visit(e, carry):
        @pl.when(place >= e)
        def _():
            block = me - 2 * e
            arrive(block)

            @pl.when(above)
            def _():
                start(block, 0, me + 2)

            start(block, 1, pair)
            fold(block)

        @pl.when((place >= e - 1) & ((e > 1) | (side == 1)))
        def _():
            block = pair - 2 * (e - 1)
            arrive(block)
            fold(block)

        @pl.when(e == jnp.maximum(place, 1))
        def _():
            for one in pair_weights():
                one.start()
            down_own(0, pair).start()

        return carry

    lax.fori_loop(1, depth + 1, visit, 0)

    for o in range(1, depth):

        @pl.when(place + o < depth)
        def _():
            down_own(o, column(o)).start()

    for h in range(group):
        cut = slice(h * seq, (h + 1) * seq)
        head = accum[0, cut, :] / total[0, cut, :] - lam[h] * (
            accum[1, cut, :] / total[1, cut, :]
        )
        head = head * lax.rsqrt(jnp.mean(head * head, axis=-1, keepdims=True) + 1e-05)
        size = head.shape[1]
        rows_in[:, h * size : (h + 1) * size] = head.astype(jnp.bfloat16)

    for o in range(half):
        base = 2 * ((far + o) % half)
        for which, parity in enumerate((1 - core, core)):
            begin = pl.multiple_of((base + parity) * rows, rows)
            order[which, o * rows : (o + 1) * rows, :] = rows_in[pl.ds(begin, rows), :]

    first = [
        mesh_copy(out_one.at[i], in_one.at[i], send_one.at[i], recv_one.at[i], "tp", partner)
        for i in range(pieces)
    ]
    second = [
        [
            mesh_copy(
                out_two.at[o, i],
                in_two.at[o, i],
                send_two.at[o, i],
                recv_two.at[o, i],
                "tp",
                fars(o + 1),
            )
            for o in range(half - 1)
        ]
        for i in range(pieces)
    ]
    span = width // pieces
    loads[0].wait()
    for i in range(pieces):
        out_one[i] = jnp.dot(
            order[0], w[:, i * span : (i + 1) * span], preferred_element_type=jnp.float32
        ).astype(jnp.bfloat16)
        first[i].start()
    kept = []
    for i in range(pieces):
        sums = jnp.dot(
            order[1], w[:, i * span : (i + 1) * span], preferred_element_type=jnp.float32
        )
        first[i].wait_recv()
        sums = sums + in_one[i].astype(jnp.float32)
        for o in range(half - 1):
            out_two[o, i] = sums[(o + 1) * rows : (o + 2) * rows].astype(jnp.bfloat16)
            second[i][o].start()
        kept.append(sums[:rows])
    squares = jnp.zeros((rows, 1), jnp.float32)
    for i in range(pieces):
        cut = slice(i * span, (i + 1) * span)
        sums = kept[i]
        for o in range(half - 1):
            second[i][o].wait_recv()
            sums = sums + in_two[o, i].astype(jnp.float32)
        sums = (stream[:, cut].astype(jnp.float32) + sums).astype(jnp.bfloat16)
        resid[:, cut] = sums
        sums = sums.astype(jnp.float32)
        squares = squares + jnp.sum(sums * sums, axis=-1, keepdims=True)
    shrink = lax.rsqrt(squares / width + 1e-06)
    for i in range(pieces):
        cut = slice(i * span, (i + 1) * span)
        gathered[place, :, cut] = (
            resid[:, cut].astype(jnp.float32) * shrink * gain[:, cut]
        ).astype(jnp.bfloat16)

    def row_copy(spot, way, target):
        return mesh_copy(
            gathered.at[spot],
            gathered.at[spot],
            send_x.at[way, spot],
            recv_x.at[spot],
            "sp",
            target,
        )

    def beside_own(way, target):
        return mesh_copy(
            gathered.at[place], beside.at[mine], send_b.at[way], recv_b.at[mine], "tp", target
        )

    def beside_on(o, u):
        return mesh_copy(
            beside.at[u], beside.at[u], send_b.at[half + o - 1], recv_b.at[u], "tp", partner
        )

    @pl.when(above)
    def _():
        row_copy(place, 0, me + 2).start()

    @pl.when(below)
    def _():
        row_copy(place, 1, me - 2).start()

    for o in range(1, half):
        beside_own(o, fars(o)).start()
    beside_own(0, partner).start()

    for one, onward in zip(pair_weights(), pair_weights_on(share_at)):
        one.wait_recv()
        onward.start()
    for o in range(1, half):
        u = fars(o)
        sd_on(o, u).wait_recv()
        sd_on(o, u).start()

    def hidden_of(block_rows, g, u):
        gate_part = jnp.dot(block_rows, g, preferred_element_type=jnp.float32)
        up_part = jnp.dot(block_rows, u, preferred_element_type=jnp.float32)
        return (gate_part / (1.0 + jnp.exp(-gate_part)) * up_part).astype(jnp.bfloat16)

    for i in range(1, 5):
        loads[i].wait()
    in_sh[mine] = hidden_of(gathered[place], s_gate[...], s_up[...])
    in_hid[place, side] = hidden_of(gathered[place], gates[0], ups[0])
    for one in pair_weights_on(other_at):
        one.wait_recv()
    in_hid[place, 1 - side] = hidden_of(gathered[place], gates[1], ups[1])

    def hid_copy(spot):
        return mesh_copy(
            out_hid.at[spot], in_hid.at[place], send_h.at[spot], recv_h.at[place], "sp",
            2 * spot + side,
        )

    def serve(spot):
        out_hid[spot, side] = hidden_of(gathered[spot], gates[0], ups[0])
        out_hid[spot, 1 - side] = hidden_of(gathered[spot], gates[1], ups[1])
        hid_copy(spot).start()

    def sh_copy(u):
        return mesh_copy(
            out_sh.at[u], in_sh.at[mine], send_s.at[u], recv_s.at[mine], "tp", u
        )

    def answer(u):
        out_sh[u] = hidden_of(beside[u], s_gate[...], s_up[...])
        sh_copy(u).start()

    def pass_down(block):
        down_pair(block).wait_recv()
        down_pair(block).start()
        down_core(block, core).start()

    down_pair(pair).wait_recv()
    down_core(pair, core).start()

    def turn(e, carry):
        low, high = place >= e, place + e < depth

        @pl.when(low)
        def _():
            row_copy(place - e, 0, pair).wait_recv()

            @pl.when(above)
            def _():
                row_copy(place - e, 0, me + 2).start()

        @pl.when(high)
        def _():
            row_copy(place + e, 0, pair).wait_recv()

            @pl.when(below)
            def _():
                row_copy(place + e, 1, me - 2).start()

        @pl.when(low)
        def _():
            pass_down(me - 2 * e)
            serve(place - e)

        @pl.when(high)
        def _():
            pass_down(me + 2 * e)
            serve(place + e)

        @pl.when(e == 1)
        def _():
            for o in range(1, half):
                u = fars(o)
                beside_on(o, u).wait_recv()
                beside_on(o, u).start()
                answer(u)
            for o in range(half):
                u = 2 * ((far + o) % half) + 1 - core
                beside_on(1, u).wait_recv()
                answer(u)

        return carry

    lax.fori_loop(1, depth, turn, 0)

    def collect(block, carry):
        @pl.when((block % 2 != side) & (block != pair))
        def _():
            down_pair(block).wait_recv()
            down_core(block, core).start()

        return carry

    lax.fori_loop(0, n, collect, 0)

    for o in range(1, depth):
        spot = (place + o) % depth
        mesh_copy(
            out_hid.at[spot], in_hid.at[spot], send_h.at[spot], recv_h.at[spot], "sp",
            2 * spot + side,
        ).wait_recv()
    for o in range(1, nt):
        u = (mine + o) % nt
        mesh_copy(
            out_sh.at[u], in_sh.at[u], send_s.at[u], recv_s.at[u], "tp", u
        ).wait_recv()
    for j in range(n):
        units[:, j * hid : (j + 1) * hid] = (
            in_hid[j // 2, j % 2].astype(jnp.float32) * mix[:, j : j + 1]
        ).astype(jnp.bfloat16)
    for j in range(nt):
        units[:, n * hid + j * wide : n * hid + (j + 1) * wide] = in_sh[j]

    loads[5].wait()
    loads[6].wait()
    for o in range(half):
        sd_on(1, 2 * ((far + o) % half) + 1 - core).wait_recv()

    def receive_down(block, carry):
        @pl.when(block != me)
        def _():
            down_core(block, 1 - core).wait_recv()

        return carry

    lax.fori_loop(0, n, receive_down, 0)
    for i in range(2 * pieces):
        cut = slice(i * span // 2, (i + 1) * span // 2)
        out[:, cut] = (
            resid[:, cut].astype(jnp.float32)
            + jnp.dot(units[...], wall[:, cut], preferred_element_type=jnp.float32)
        ).astype(jnp.bfloat16)

    def settle(e, carry):
        @pl.when(place >= e)
        def _():
            block = me - 2 * e

            @pl.when(above)
            def _():
                for one in copies(block, 0, me + 2, False):
                    one.wait_send()
                row_copy(place - e, 0, me + 2).wait_send()

            @pl.when((e > 0) | (side == 0))
            def _():
                for one in copies(block, 1, pair, False):
                    one.wait_send()

        @pl.when((place + e < depth) & below)
        def _():
            row_copy(place + e, 1, me - 2).wait_send()

        @pl.when(e != place)
        def _():
            hid_copy(e).wait_send()
            down_pair(2 * e + side).wait_send()

        return carry

    lax.fori_loop(0, depth, settle, 0)

    def settle_down(block, carry):
        @pl.when(block != me)
        def _():
            down_core(block, core).wait_send()

        return carry

    lax.fori_loop(0, n, settle_down, 0)
    for i in range(pieces):
        first[i].wait_send()
        for o in range(half - 1):
            second[i][o].wait_send()
    for one in pair_weights() + pair_weights_on(share_at):
        one.wait_send()
    for o in range(1, depth):
        down_own(o, column(o)).wait_send()
    down_own(0, pair).wait_send()
    sd_own(0, partner).wait_send()
    beside_own(0, partner).wait_send()
    for o in range(1, half):
        u = fars(o)
        sd_own(o, u).wait_send()
        sd_on(o, u).wait_send()
        beside_own(o, u).wait_send()
        beside_on(o, u).wait_send()
    for o in range(1, nt):
        sh_copy((mine + o) % nt).wait_send()


def near(
    stream_in,
    q_first,
    q_second,
    k_first,
    k_second,
    values,
    head_lambda,
    w_out,
    norm_gain,
    routes,
    route_w,
    w_gate,
    w_up,
    w_down,
    s_gate,
    s_up,
    s_down,
):
    n, nt = lax.axis_size("sp"), lax.axis_size("tp")
    depth, half = n // 2, nt // 2
    seq, rows, width = q_first.shape[0], stream_in.shape[0], stream_in.shape[1]
    group, value_dim = q_first.shape[1] // HEAD, values.shape[1]
    hid, wide = w_down.shape[1], s_down.shape[0]
    tall, features = group * seq, group * value_dim
    pieces = 4
    span = width // pieces
    chosen = routes[:, :, None] == jnp.arange(n, dtype=jnp.int32)[None, None, :]
    mix = jnp.sum(jnp.where(chosen, route_w[:, :, None], 0.0), axis=1)
    vmem = pl.BlockSpec(memory_space=pltpu.VMEM)
    smem = pl.BlockSpec(memory_space=pltpu.SMEM)
    hbm = pl.BlockSpec(memory_space=pl.ANY)
    low, high = jnp.bfloat16, jnp.float32
    dma = pltpu.SemaphoreType.DMA
    return pl.pallas_call(
        functools.partial(near_kernel, n, nt, group, pieces),
        out_shape=jax.ShapeDtypeStruct((rows, width), low),
        in_specs=[vmem] * 5 + [smem, hbm] + [vmem] * 3 + [hbm] * 6,
        out_specs=vmem,
        scratch_shapes=[
            pltpu.VMEM((2, tall, HEAD), low),
            pltpu.VMEM((n, seq, HEAD), low),
            pltpu.VMEM((n, seq, HEAD), low),
            pltpu.VMEM((n, seq, value_dim), low),
            pltpu.VMEM((2, tall, 1), high),
            pltpu.VMEM((2, tall, 1), high),
            pltpu.VMEM((2, tall, value_dim), high),
            pltpu.VMEM((seq, features), low),
            pltpu.VMEM((features, width), low),
            pltpu.VMEM((2, half * rows, features), low),
            pltpu.VMEM((pieces, half * rows, span), low),
            pltpu.VMEM((pieces, half * rows, span), low),
            pltpu.VMEM((half - 1, pieces, rows, span), low),
            pltpu.VMEM((half - 1, pieces, rows, span), low),
            pltpu.VMEM((rows, width), low),
            pltpu.VMEM((2, width, hid), low),
            pltpu.VMEM((2, width, hid), low),
            pltpu.VMEM((width, wide), low),
            pltpu.VMEM((width, wide), low),
            pltpu.VMEM((n * hid + nt * wide, width), low),
            pltpu.VMEM((depth, rows, width), low),
            pltpu.VMEM((nt, rows, width), low),
            pltpu.VMEM((depth, 2, rows, hid), low),
            pltpu.VMEM((depth, 2, rows, hid), low),
            pltpu.VMEM((nt, rows, wide), low),
            pltpu.VMEM((nt, rows, wide), low),
            pltpu.VMEM((rows, n * hid + nt * wide), low),
            dma((7,)),
            dma((2, 3, n)),
            dma((3, n)),
            dma((pieces,)),
            dma((pieces,)),
            dma((half - 1, pieces)),
            dma((half - 1, pieces)),
            dma((2, 2)),
            dma((2, 2)),
            dma((depth + 2 * n,)),
            dma((2, n)),
            dma((nt,)),
            dma((nt,)),
            dma((2, depth)),
            dma((depth,)),
            dma((nt,)),
            dma((nt,)),
            dma((depth,)),
            dma((depth,)),
            dma((nt,)),
            dma((nt,)),
        ],
        compiler_params=pltpu.CompilerParams(
            collective_id=0, has_side_effects=True, vmem_limit_bytes=60 << 20
        ),
        name="layer",
    )(
        q_first, q_second, k_first, k_second, values, head_lambda, w_out, stream_in,
        norm_gain.reshape(1, width), mix, w_gate[0], w_up[0], s_gate, s_up, w_down[0], s_down,
    )


def layer(*arrays):
    n, nt = lax.axis_size("sp"), lax.axis_size("tp")
    k_first, values, w_gate, w_down, s_down = (arrays[i] for i in (3, 5, 11, 13, 16))
    fits = (
        2 <= n <= 16
        and n % 2 == 0
        and nt >= 4
        and nt % 2 == 0
        and k_first.shape[1] == HEAD
        and w_gate.shape[0] == 1
        and w_down.shape[1] % (16 * nt) == 0
        and s_down.shape[0] % (16 * n) == 0
    )
    return near(*arrays) if fits else local(*arrays)


def solution(mesh):
    return jax.shard_map(
        layer,
        mesh=mesh,
        in_specs=(
            P(("sp", "tp"), None),
            P("sp", "tp"),
            P("sp", "tp"),
            P("sp", "tp"),
            P("sp", "tp"),
            P("sp", "tp"),
            P("tp"),
            P("tp", None),
            P(),
            P(("sp", "tp"), None),
            P(("sp", "tp"), None),
            P("sp", None, None),
            P("sp", None, None),
            P("sp", None, None),
            P(None, "tp"),
            P(None, "tp"),
            P("tp", None),
        ),
        out_specs=P(("sp", "tp"), None),
        check_vma=False,
    )
```

```python
import functools
import math

import jax
import jax.numpy as jnp
from jax import lax
from jax.experimental import pallas as pl
from jax.experimental.pallas import tpu as pltpu
from jax.sharding import PartitionSpec as P

HEAD = 128


FLOOR = -1e30


def absorb(state, first_q, second_q, first_k, second_k, value_rows, query_pos, key_pos):
    allowed = key_pos[None, :] <= query_pos[:, None]
    scale = first_q.shape[-1] ** (-0.5)
    result = []
    pairs = ((first_q, first_k), (second_q, second_k))
    for index in range(2):
        query_rows, key_rows = pairs[index]
        peak, total, accum = (state[3 * index], state[3 * index + 1], state[3 * index + 2])
        scores = (
            jnp.einsum("qagd,kad->agqk", query_rows, key_rows, preferred_element_type=jnp.float32)
            * scale
        )
        scores = jnp.where(allowed, scores, FLOOR)
        raised = jnp.maximum(peak, scores.max(-1))
        weights = jnp.where(allowed, jnp.exp(scores - raised[..., None]), 0.0)
        fade = jnp.exp(peak - raised)
        total = total * fade + weights.sum(-1)
        accum = accum * fade[..., None] + jnp.einsum(
            "agqk,kad->agqd",
            weights.astype(jnp.bfloat16),
            value_rows,
            preferred_element_type=jnp.float32,
        )
        result += [raised, total, accum]
    return tuple(result)


def empty_state(kv_local, group, count, value_dim):
    peaks = jnp.full((kv_local, group, count), FLOOR, jnp.float32)
    sums = jnp.zeros((kv_local, group, count), jnp.float32)
    accums = jnp.zeros((kv_local, group, count, value_dim), jnp.float32)
    return (peaks, sums, accums, peaks, sums, accums)


def fold_rows(state, first_q, second_q, query_pos, last_row, pieces, start):
    first_k, second_k, value_rows = pieces
    length = first_k.shape[0]
    kv_local = first_q.shape[1]
    value_dim = value_rows.shape[1] // kv_local
    span = math.gcd(length, 2048)

    def sweep(current):

        def visit(block, inner):
            begin = block * span
            key_one = lax.dynamic_slice_in_dim(first_k, begin, span, 0).reshape(
                span, kv_local, HEAD
            )
            key_two = lax.dynamic_slice_in_dim(second_k, begin, span, 0).reshape(
                span, kv_local, HEAD
            )
            value_part = lax.dynamic_slice_in_dim(value_rows, begin, span, 0).reshape(
                span, kv_local, value_dim
            )
            key_pos = begin + jnp.arange(span, dtype=jnp.int32)
            return absorb(
                inner, first_q, second_q, key_one, key_two, value_part, query_pos, key_pos
            )

        return lax.fori_loop(0, length // span, visit, current)

    def unchanged(current):
        return current

    return lax.cond(start <= last_row, sweep, unchanged, state)


def finish_heads(final, head_lambda):
    kv_local, group, count, value_dim = final[2].shape
    weight = head_lambda.reshape(kv_local, group, 1, 1)
    head_out = final[2] / final[1][..., None] - weight * final[5] / final[4][..., None]
    head_out = head_out * lax.rsqrt(jnp.mean(head_out * head_out, axis=-1, keepdims=True) + 1e-05)
    return (
        head_out.transpose(2, 0, 1, 3)
        .reshape(count, kv_local * group * value_dim)
        .astype(jnp.bfloat16)
    )


def shared_part(normed, s_gate, s_up, s_down):
    piece = lax.all_gather(normed, "tp", axis=0, tiled=True)
    gate_part = jnp.dot(piece, s_gate, preferred_element_type=jnp.float32)
    up_part = jnp.dot(piece, s_up, preferred_element_type=jnp.float32)
    hidden = (jax.nn.silu(gate_part) * up_part).astype(jnp.bfloat16)
    terms = jnp.dot(hidden, s_down, preferred_element_type=jnp.float32)
    return lax.psum_scatter(
        terms.astype(jnp.bfloat16), "tp", scatter_dimension=0, tiled=True
    ).astype(jnp.float32)


def routed_part(normed, routes, route_w, w_gate, w_up, w_down):
    rows, topk = routes.shape
    local_experts = w_gate.shape[0]
    experts = local_experts * lax.axis_size("sp")
    slots = max(2, 3 * rows * topk // (2 * experts))
    flat_ids = routes.reshape(-1)
    hits = (flat_ids[:, None] == jnp.arange(experts, dtype=jnp.int32)[None, :]).astype(jnp.int32)
    slot_of = jnp.sum(jnp.cumsum(hits, axis=0) * hits, axis=1) - 1
    target = flat_ids * slots + slot_of
    placing = jnp.any(
        jnp.arange(experts * slots, dtype=jnp.int32)[:, None, None]
        == target.reshape(rows, topk)[None, :, :],
        axis=-1,
    ).astype(jnp.bfloat16)
    outgoing = (
        jnp.dot(placing, normed, preferred_element_type=jnp.float32)
        .astype(jnp.bfloat16)
        .reshape(experts, slots, normed.shape[1])
    )
    arrived = lax.all_to_all(outgoing, "sp", split_axis=0, concat_axis=0, tiled=True)
    sources = arrived.shape[0] // local_experts
    grouped = arrived.reshape(sources, local_experts, arrived.shape[1], arrived.shape[2])
    gate_part = jnp.einsum("sjcd,jdf->sjcf", grouped, w_gate, preferred_element_type=jnp.float32)
    up_part = jnp.einsum("sjcd,jdf->sjcf", grouped, w_up, preferred_element_type=jnp.float32)
    hidden = (jax.nn.silu(gate_part) * up_part).astype(jnp.bfloat16)
    result = jnp.einsum(
        "sjcf,jfd->sjcd", hidden, w_down, preferred_element_type=jnp.float32
    ).astype(jnp.bfloat16)
    returned = lax.all_to_all(
        result.reshape(arrived.shape), "sp", split_axis=0, concat_axis=0, tiled=True
    )
    picked = (
        returned.reshape(experts * slots, normed.shape[1])[target]
        .reshape(rows, topk, normed.shape[1])
        .astype(jnp.float32)
    )
    return jnp.sum(picked * route_w[..., None], axis=1)


def local(
    stream_in,
    q_first,
    q_second,
    k_first,
    k_second,
    values,
    head_lambda,
    w_out,
    norm_gain,
    routes,
    route_w,
    w_gate,
    w_up,
    w_down,
    s_gate,
    s_up,
    s_down,
):
    seq_rows = q_first.shape[0]
    kv_local = k_first.shape[1] // HEAD
    heads_local = q_first.shape[1] // HEAD
    group = heads_local // kv_local
    value_dim = values.shape[1] // kv_local
    offset = lax.axis_index("sp") * seq_rows
    query_pos = offset + jnp.arange(seq_rows, dtype=jnp.int32)
    last_row = offset + seq_rows - 1
    first_q = q_first.reshape(seq_rows, kv_local, group, HEAD)
    second_q = q_second.reshape(seq_rows, kv_local, group, HEAD)
    start_state = empty_state(kv_local, group, seq_rows, value_dim)
    folded_state = fold_rows(
        start_state,
        first_q,
        second_q,
        query_pos,
        last_row,
        (
            lax.all_gather(k_first, "sp", axis=0, tiled=True),
            lax.all_gather(k_second, "sp", axis=0, tiled=True),
            lax.all_gather(values, "sp", axis=0, tiled=True),
        ),
        jnp.int32(0),
    )
    attn_rows = finish_heads(folded_state, head_lambda)
    attn = lax.psum_scatter(
        jnp.dot(attn_rows, w_out, preferred_element_type=jnp.float32).astype(jnp.bfloat16),
        "tp",
        scatter_dimension=0,
        tiled=True,
    ).astype(jnp.float32)
    resid = (stream_in.astype(jnp.float32) + attn).astype(jnp.bfloat16)
    stream = lax.optimization_barrier(resid).astype(jnp.float32)
    normed = (
        stream * lax.rsqrt(jnp.mean(stream * stream, axis=-1, keepdims=True) + 1e-06) * norm_gain
    ).astype(jnp.bfloat16)
    routed = routed_part(normed, routes, route_w, w_gate, w_up, w_down)
    shared = shared_part(normed, s_gate, s_up, s_down)
    return (stream + routed + shared).astype(jnp.bfloat16)


def mesh_copy(src, dst, send_sem, recv_sem, axis, target):
    return pltpu.make_async_remote_copy(
        src_ref=src,
        dst_ref=dst,
        send_sem=send_sem,
        recv_sem=recv_sem,
        device_id={axis: target},
        device_id_type=pl.DeviceIdType.MESH,
    )


def greet(axis, target):
    pl.semaphore_signal(
        pltpu.get_barrier_semaphore(),
        inc=1,
        device_id={axis: target},
        device_id_type=pl.DeviceIdType.MESH,
    )


def near_kernel(
    n, nt, group, pieces,
    q_one, q_two, k_one, k_two, val, lam, w_out_h, stream, gain, mix,
    gate_h, up_h, s_gate_h, s_up_h, down_h, s_down_h,
    out,
    stacked, keys_one, keys_two, vals, peak, total, accum, rows_in,
    w, order, out_one, in_one, out_two, in_two, resid,
    gates, ups, s_gate, s_up, wall, gathered, beside, out_hid, in_hid, out_sh, in_sh, units,
    load, send_kv, recv_kv, send_one, recv_one, send_two, recv_two,
    send_g, recv_g, send_d, recv_d, send_sd, recv_sd,
    send_x, recv_x, send_b, recv_b, send_h, recv_h, send_s, recv_s,
):
    me, mine = lax.axis_index("sp"), lax.axis_index("tp")
    place, side = me // 2, me % 2
    far, core = mine // 2, mine % 2
    depth, half = n // 2, nt // 2
    pair, partner = me + 1 - 2 * side, mine + 1 - 2 * core
    above, below = place < depth - 1, place > 0
    seq = q_one.shape[0]
    rows, width = stream.shape
    hid, wide = down_h.shape[0], s_down_h.shape[0]
    scale = HEAD ** (-0.5)

    def fars(o):
        return 2 * ((far + o) % half) + core

    def column(o):
        return 2 * ((place + o) % depth) + side

    loads = [
        pltpu.make_async_copy(source, target, load.at[i])
        for i, (source, target) in enumerate(
            (
                (w_out_h, w),
                (gate_h, gates.at[0]),
                (up_h, ups.at[0]),
                (s_gate_h, s_gate),
                (s_up_h, s_up),
                (down_h, wall.at[pl.ds(pl.multiple_of(me * hid, hid), hid)]),
                (s_down_h, wall.at[pl.ds(pl.multiple_of(n * hid + mine * wide, wide), wide)]),
            )
        )
    ]
    for o in range(1, depth):
        greet("sp", column(o))
    greet("sp", pair)
    for o in range(1, half):
        greet("tp", fars(o))
    greet("tp", partner)
    pl.semaphore_wait(pltpu.get_barrier_semaphore(), depth + half)

    sources = (k_one, k_two, val)
    held = (keys_one, keys_two, vals)

    def copies(block, way, target, own):
        return [
            mesh_copy(
                sources[a] if own else held[a].at[block],
                held[a].at[block],
                send_kv.at[way, a, block],
                recv_kv.at[a, block],
                "sp",
                target,
            )
            for a in range(3)
        ]

    def start(block, way, target, own=False):
        for one in copies(block, way, target, own):
            one.start()

    def arrive(block):
        for one in copies(block, 0, pair, False):
            one.wait_recv()

    share = width // 2
    share_at = pl.ds(pl.multiple_of(core * share, share), share)
    other_at = pl.ds(pl.multiple_of((1 - core) * share, share), share)

    def pair_weights():
        return [
            mesh_copy(
                h.at[share_at], v.at[1, share_at], send_g.at[0, i], recv_g.at[0, i], "sp", pair
            )
            for i, (h, v) in enumerate(((gate_h, gates), (up_h, ups)))
        ]

    def pair_weights_on(at):
        return [
            mesh_copy(
                v.at[1, at], v.at[1, at], send_g.at[1, i], recv_g.at[1, i], "tp", partner
            )
            for i, v in enumerate((gates, ups))
        ]

    part = hid // 2

    def down_at(block, c):
        return wall.at[pl.ds(pl.multiple_of(block * hid + c * part, part), part)]

    def down_own(way, target, axis="sp"):
        return mesh_copy(
            down_h.at[pl.ds(pl.multiple_of(core * part, part), part)],
            down_at(me, core),
            send_d.at[way],
            recv_d.at[0, me],
            axis,
            target,
        )

    def down_pair(block):
        return mesh_copy(
            down_at(block, core),
            down_at(block, core),
            send_d.at[depth + block],
            recv_d.at[0, block],
            "sp",
            pair,
        )

    def down_core(block, c):
        return mesh_copy(
            down_at(block, c),
            down_at(block, c),
            send_d.at[depth + n + block],
            recv_d.at[1, block],
            "tp",
            partner,
        )

    def sd_at(u):
        return wall.at[pl.ds(pl.multiple_of(n * hid + u * wide, wide), wide)]

    def sd_own(way, target):
        return mesh_copy(s_down_h, sd_at(mine), send_sd.at[way], recv_sd.at[mine], "tp", target)

    def sd_on(o, u):
        return mesh_copy(
            sd_at(u), sd_at(u), send_sd.at[half + o - 1], recv_sd.at[u], "tp", partner
        )

    @pl.when(above)
    def _():
        start(me, 0, me + 2, True)

    @pl.when(side == 0)
    def _():
        start(me, 1, pair, True)

    for one in loads:
        one.start()
    for o in range(1, half):
        sd_own(o, fars(o)).start()
    sd_own(0, partner).start()
    for o in range(1, depth):

        @pl.when(place + o >= depth)
        def _():
            down_own(o, column(o)).start()

    for index, q in enumerate((q_one, q_two)):
        for h in range(group):
            stacked[index, h * seq : (h + 1) * seq, :] = q[:, h * HEAD : (h + 1) * HEAD]

    def scores_of(index, keys):
        return (
            lax.dot_general(
                stacked[index], keys, (((1,), (1,)), ((), ())), preferred_element_type=jnp.float32
            )
            * scale
        )

    spread = (group * seq, seq)
    row_of = lax.broadcasted_iota(jnp.int32, spread, 0) % seq
    allowed = lax.broadcasted_iota(jnp.int32, spread, 1) <= row_of
    for index, keys in enumerate((k_one, k_two)):
        scores = jnp.where(allowed, scores_of(index, keys[...]), FLOOR)
        top = jnp.max(scores, axis=-1, keepdims=True)
        weights = jnp.exp(scores - top)
        peak[index] = top
        total[index] = jnp.sum(weights, axis=-1, keepdims=True)
        accum[index] = jnp.dot(
            weights.astype(jnp.bfloat16), val[...], preferred_element_type=jnp.float32
        )

    def fold(block):
        for index in range(2):
            scores = scores_of(index, held[index][block])
            old = peak[index]
            top = jnp.maximum(old, jnp.max(scores, axis=-1, keepdims=True))
            weights = jnp.exp(scores - top)
            fade = jnp.exp(old - top)
            peak[index] = top
            total[index] = total[index] * fade + jnp.sum(weights, axis=-1, keepdims=True)
            accum[index] = accum[index] * fade + jnp.dot(
                weights.astype(jnp.bfloat16), vals[block], preferred_element_type=jnp.float32
            )

    def visit(e, carry):
        @pl.when(place >= e)
        def _():
            block = me - 2 * e
            arrive(block)

            @pl.when(above)
            def _():
                start(block, 0, me + 2)

            start(block, 1, pair)
            fold(block)

        @pl.when((place >= e - 1) & ((e > 1) | (side == 1)))
        def _():
            block = pair - 2 * (e - 1)
            arrive(block)
            fold(block)

        @pl.when(e == jnp.maximum(place, 1))
        def _():
            for one in pair_weights():
                one.start()
            down_own(0, pair).start()

        return carry

    lax.fori_loop(1, depth + 1, visit, 0)

    @pl.when(above)
    def _():
        down_own(1, me + 2).start()

    def down_up(block):
        return mesh_copy(
            down_at(block, core),
            down_at(block, core),
            send_d.at[depth + 2 * n + block],
            recv_d.at[0, block],
            "sp",
            me + 2,
        )

    def lift(d):
        @pl.when((place >= d) & above)
        def _():
            down_up(me - 2 * d).wait_recv()
            down_up(me - 2 * d).start()

    for h in range(group):
        cut = slice(h * seq, (h + 1) * seq)
        head = accum[0, cut, :] / total[0, cut, :] - lam[h] * (
            accum[1, cut, :] / total[1, cut, :]
        )
        head = head * lax.rsqrt(jnp.mean(head * head, axis=-1, keepdims=True) + 1e-05)
        size = head.shape[1]
        rows_in[:, h * size : (h + 1) * size] = head.astype(jnp.bfloat16)

    for o in range(half):
        base = 2 * ((far + o) % half)
        for which, parity in enumerate((1 - core, core)):
            begin = pl.multiple_of((base + parity) * rows, rows)
            order[which, o * rows : (o + 1) * rows, :] = rows_in[pl.ds(begin, rows), :]

    first = [
        mesh_copy(out_one.at[i], in_one.at[i], send_one.at[i], recv_one.at[i], "tp", partner)
        for i in range(pieces)
    ]
    second = [
        [
            mesh_copy(
                out_two.at[o, i],
                in_two.at[o, i],
                send_two.at[o, i],
                recv_two.at[o, i],
                "tp",
                fars(o + 1),
            )
            for o in range(half - 1)
        ]
        for i in range(pieces)
    ]
    span = width // pieces
    loads[0].wait()
    for i in range(pieces):
        out_one[i] = jnp.dot(
            order[0], w[:, i * span : (i + 1) * span], preferred_element_type=jnp.float32
        ).astype(jnp.bfloat16)
        first[i].start()
    lift(1)
    kept = []
    for i in range(pieces):
        sums = jnp.dot(
            order[1], w[:, i * span : (i + 1) * span], preferred_element_type=jnp.float32
        )
        first[i].wait_recv()
        sums = sums + in_one[i].astype(jnp.float32)
        for o in range(half - 1):
            out_two[o, i] = sums[(o + 1) * rows : (o + 2) * rows].astype(jnp.bfloat16)
            second[i][o].start()
        kept.append(sums[:rows])
    for d in range(2, depth):
        lift(d)
    for o in range(1, half):
        u = fars(o)
        sd_on(o, u).wait_recv()
        sd_on(o, u).start()
    squares = jnp.zeros((rows, 1), jnp.float32)
    for i in range(pieces):
        cut = slice(i * span, (i + 1) * span)
        sums = kept[i]
        for o in range(half - 1):
            second[i][o].wait_recv()
            sums = sums + in_two[o, i].astype(jnp.float32)
        sums = (stream[:, cut].astype(jnp.float32) + sums).astype(jnp.bfloat16)
        resid[:, cut] = sums
        sums = sums.astype(jnp.float32)
        squares = squares + jnp.sum(sums * sums, axis=-1, keepdims=True)
    shrink = lax.rsqrt(squares / width + 1e-06)
    for i in range(pieces):
        cut = slice(i * span, (i + 1) * span)
        gathered[place, :, cut] = (
            resid[:, cut].astype(jnp.float32) * shrink * gain[:, cut]
        ).astype(jnp.bfloat16)

    chunk = rows // 2

    def row_copy(spot, way, target, c):
        some = gathered.at[spot, pl.ds(c * chunk, chunk)]
        return mesh_copy(
            some,
            some,
            send_x.at[way, c, spot],
            recv_x.at[c, spot],
            "sp",
            target,
        )

    def beside_own(way, target):
        return mesh_copy(
            gathered.at[place], beside.at[mine], send_b.at[way], recv_b.at[mine], "tp", target
        )

    def beside_on(o, u):
        return mesh_copy(
            beside.at[u], beside.at[u], send_b.at[half + o - 1], recv_b.at[u], "tp", partner
        )

    for c in range(2):
        pl.when(above)(lambda: row_copy(place, 0, me + 2, c).start())
        pl.when(below)(lambda: row_copy(place, 1, me - 2, c).start())

    for o in range(1, half):
        beside_own(o, fars(o)).start()
    beside_own(0, partner).start()

    def pass_down(e):
        def one(block, fresh):
            pl.when(fresh)(lambda: down_pair(block).wait_recv())
            down_pair(block).start()
            down_core(block, core).start()

        pl.when(place >= e)(lambda: one(me - 2 * e, jnp.logical_not(above)))
        pl.when(place + e < depth)(lambda: one(me + 2 * e, place >= 0))

    def collect(e):
        def one(block):
            down_pair(block).wait_recv()
            down_core(block, core).start()

        pl.when(place >= e)(lambda: one(pair - 2 * e))
        pl.when(place + e < depth)(lambda: one(pair + 2 * e))

    for one, onward in zip(pair_weights(), pair_weights_on(share_at)):
        one.wait_recv()
        onward.start()
    pass_down(1)
    def hidden_of(block_rows, g, u):
        gate_part = jnp.dot(block_rows, g, preferred_element_type=jnp.float32)
        up_part = jnp.dot(block_rows, u, preferred_element_type=jnp.float32)
        return (gate_part / (1.0 + jnp.exp(-gate_part)) * up_part).astype(jnp.bfloat16)

    for i in range(1, 5):
        loads[i].wait()
    in_sh[mine] = hidden_of(gathered[place], s_gate[...], s_up[...])
    in_hid[place, side] = hidden_of(gathered[place], gates[0], ups[0])

    def hid_copy(spot):
        return mesh_copy(
            out_hid.at[spot], in_hid.at[place], send_h.at[spot], recv_h.at[place], "sp",
            2 * spot + side,
        )

    def serve(spot):
        out_hid[spot, side] = hidden_of(gathered[spot], gates[0], ups[0])
        out_hid[spot, 1 - side] = hidden_of(gathered[spot], gates[1], ups[1])
        hid_copy(spot).start()

    def sh_copy(u):
        return mesh_copy(
            out_sh.at[u], in_sh.at[mine], send_s.at[u], recv_s.at[mine], "tp", u
        )

    def answer(u):
        out_sh[u] = hidden_of(beside[u], s_gate[...], s_up[...])
        sh_copy(u).start()

    def turn(e, carry):
        low, high = place >= e, place + e < depth

        for c in range(2):

            @pl.when(low)
            def _():
                row_copy(place - e, 0, pair, c).wait_recv()
                pl.when(above)(lambda: row_copy(place - e, 0, me + 2, c).start())

            @pl.when(high)
            def _():
                row_copy(place + e, 0, pair, c).wait_recv()
                pl.when(below)(lambda: row_copy(place + e, 1, me - 2, c).start())

        pass_down(e + 1)

        @pl.when(e == 1)
        def _():
            down_pair(pair).wait_recv()
            down_core(pair, core).start()
            for one in pair_weights_on(other_at):
                one.wait_recv()

        @pl.when(low)
        def _():
            serve(place - e)

        @pl.when(high)
        def _():
            serve(place + e)

        @pl.when(e > 1)
        def _():
            collect(e - 1)

        @pl.when(e == 1)
        def _():
            in_hid[place, 1 - side] = hidden_of(gathered[place], gates[1], ups[1])
            for o in range(1, half):
                u = fars(o)
                beside_on(o, u).wait_recv()
                beside_on(o, u).start()
                answer(u)
            for o in range(half):
                u = 2 * ((far + o) % half) + 1 - core
                beside_on(1, u).wait_recv()
                answer(u)

        return carry

    lax.fori_loop(1, depth, turn, 0)

    collect(depth - 1)

    for o in range(1, depth):
        spot = (place + o) % depth
        mesh_copy(
            out_hid.at[spot], in_hid.at[spot], send_h.at[spot], recv_h.at[spot], "sp",
            2 * spot + side,
        ).wait_recv()
    for o in range(1, nt):
        u = (mine + o) % nt
        mesh_copy(
            out_sh.at[u], in_sh.at[u], send_s.at[u], recv_s.at[u], "tp", u
        ).wait_recv()
    for j in range(n):
        units[:, j * hid : (j + 1) * hid] = (
            in_hid[j // 2, j % 2].astype(jnp.float32) * mix[:, j : j + 1]
        ).astype(jnp.bfloat16)
    for j in range(nt):
        units[:, n * hid + j * wide : n * hid + (j + 1) * wide] = in_sh[j]

    loads[5].wait()
    loads[6].wait()
    for o in range(half):
        sd_on(1, 2 * ((far + o) % half) + 1 - core).wait_recv()

    def receive_down(block, carry):
        @pl.when(block != me)
        def _():
            down_core(block, 1 - core).wait_recv()

        return carry

    lax.fori_loop(0, n, receive_down, 0)
    for i in range(2 * pieces):
        cut = slice(i * span // 2, (i + 1) * span // 2)
        out[:, cut] = (
            resid[:, cut].astype(jnp.float32)
            + jnp.dot(units[...], wall[:, cut], preferred_element_type=jnp.float32)
        ).astype(jnp.bfloat16)

    def settle(e, carry):
        @pl.when(place >= e)
        def _():
            block = me - 2 * e

            @pl.when(above)
            def _():
                for one in copies(block, 0, me + 2, False):
                    one.wait_send()
                for c in range(2):
                    row_copy(place - e, 0, me + 2, c).wait_send()

                @pl.when(e > 0)
                def _():
                    down_up(block).wait_send()

            @pl.when((e > 0) | (side == 0))
            def _():
                for one in copies(block, 1, pair, False):
                    one.wait_send()

        @pl.when((place + e < depth) & below)
        def _():
            for c in range(2):
                row_copy(place + e, 1, me - 2, c).wait_send()

        @pl.when(e != place)
        def _():
            hid_copy(e).wait_send()
            down_pair(2 * e + side).wait_send()

        return carry

    lax.fori_loop(0, depth, settle, 0)

    def settle_down(block, carry):
        @pl.when(block != me)
        def _():
            down_core(block, core).wait_send()

        return carry

    lax.fori_loop(0, n, settle_down, 0)
    for i in range(pieces):
        first[i].wait_send()
        for o in range(half - 1):
            second[i][o].wait_send()
    for one in pair_weights() + pair_weights_on(share_at):
        one.wait_send()
    for o in range(1, depth):
        pl.when((place + o >= depth) | (o == 1))(lambda: down_own(o, column(o)).wait_send())
    down_own(0, pair).wait_send()
    sd_own(0, partner).wait_send()
    beside_own(0, partner).wait_send()
    for o in range(1, half):
        u = fars(o)
        sd_own(o, u).wait_send()
        sd_on(o, u).wait_send()
        beside_own(o, u).wait_send()
        beside_on(o, u).wait_send()
    for o in range(1, nt):
        sh_copy((mine + o) % nt).wait_send()


def near(
    stream_in,
    q_first,
    q_second,
    k_first,
    k_second,
    values,
    head_lambda,
    w_out,
    norm_gain,
    routes,
    route_w,
    w_gate,
    w_up,
    w_down,
    s_gate,
    s_up,
    s_down,
):
    n, nt = lax.axis_size("sp"), lax.axis_size("tp")
    depth, half = n // 2, nt // 2
    seq, rows, width = q_first.shape[0], stream_in.shape[0], stream_in.shape[1]
    group, value_dim = q_first.shape[1] // HEAD, values.shape[1]
    hid, wide = w_down.shape[1], s_down.shape[0]
    tall, features = group * seq, group * value_dim
    pieces = 4
    span = width // pieces
    chosen = routes[:, :, None] == jnp.arange(n, dtype=jnp.int32)[None, None, :]
    mix = jnp.sum(jnp.where(chosen, route_w[:, :, None], 0.0), axis=1)
    vmem = pl.BlockSpec(memory_space=pltpu.VMEM)
    smem = pl.BlockSpec(memory_space=pltpu.SMEM)
    hbm = pl.BlockSpec(memory_space=pl.ANY)
    low, high = jnp.bfloat16, jnp.float32
    dma = pltpu.SemaphoreType.DMA
    return pl.pallas_call(
        functools.partial(near_kernel, n, nt, group, pieces),
        out_shape=jax.ShapeDtypeStruct((rows, width), low),
        in_specs=[vmem] * 5 + [smem, hbm] + [vmem] * 3 + [hbm] * 6,
        out_specs=vmem,
        scratch_shapes=[
            pltpu.VMEM((2, tall, HEAD), low),
            pltpu.VMEM((n, seq, HEAD), low),
            pltpu.VMEM((n, seq, HEAD), low),
            pltpu.VMEM((n, seq, value_dim), low),
            pltpu.VMEM((2, tall, 1), high),
            pltpu.VMEM((2, tall, 1), high),
            pltpu.VMEM((2, tall, value_dim), high),
            pltpu.VMEM((seq, features), low),
            pltpu.VMEM((features, width), low),
            pltpu.VMEM((2, half * rows, features), low),
            pltpu.VMEM((pieces, half * rows, span), low),
            pltpu.VMEM((pieces, half * rows, span), low),
            pltpu.VMEM((half - 1, pieces, rows, span), low),
            pltpu.VMEM((half - 1, pieces, rows, span), low),
            pltpu.VMEM((rows, width), low),
            pltpu.VMEM((2, width, hid), low),
            pltpu.VMEM((2, width, hid), low),
            pltpu.VMEM((width, wide), low),
            pltpu.VMEM((width, wide), low),
            pltpu.VMEM((n * hid + nt * wide, width), low),
            pltpu.VMEM((depth, rows, width), low),
            pltpu.VMEM((nt, rows, width), low),
            pltpu.VMEM((depth, 2, rows, hid), low),
            pltpu.VMEM((depth, 2, rows, hid), low),
            pltpu.VMEM((nt, rows, wide), low),
            pltpu.VMEM((nt, rows, wide), low),
            pltpu.VMEM((rows, n * hid + nt * wide), low),
            dma((7,)),
            dma((2, 3, n)),
            dma((3, n)),
            dma((pieces,)),
            dma((pieces,)),
            dma((half - 1, pieces)),
            dma((half - 1, pieces)),
            dma((2, 2)),
            dma((2, 2)),
            dma((depth + 3 * n,)),
            dma((2, n)),
            dma((nt,)),
            dma((nt,)),
            dma((2, 2, depth)),
            dma((2, depth)),
            dma((nt,)),
            dma((nt,)),
            dma((depth,)),
            dma((depth,)),
            dma((nt,)),
            dma((nt,)),
        ],
        compiler_params=pltpu.CompilerParams(
            collective_id=0, has_side_effects=True, vmem_limit_bytes=60 << 20
        ),
        name="layer",
    )(
        q_first, q_second, k_first, k_second, values, head_lambda, w_out, stream_in,
        norm_gain.reshape(1, width), mix, w_gate[0], w_up[0], s_gate, s_up, w_down[0], s_down,
    )


def layer(*arrays):
    n, nt = lax.axis_size("sp"), lax.axis_size("tp")
    k_first, values, w_gate, w_down, s_down = (arrays[i] for i in (3, 5, 11, 13, 16))
    fits = (
        2 <= n <= 16
        and n % 2 == 0
        and nt >= 4
        and nt % 2 == 0
        and k_first.shape[1] == HEAD
        and w_gate.shape[0] == 1
        and w_down.shape[1] % (16 * nt) == 0
        and s_down.shape[0] % (16 * n) == 0
    )
    return near(*arrays) if fits else local(*arrays)


def solution(mesh):
    return jax.shard_map(
        layer,
        mesh=mesh,
        in_specs=(
            P(("sp", "tp"), None),
            P("sp", "tp"),
            P("sp", "tp"),
            P("sp", "tp"),
            P("sp", "tp"),
            P("sp", "tp"),
            P("tp"),
            P("tp", None),
            P(),
            P(("sp", "tp"), None),
            P(("sp", "tp"), None),
            P("sp", None, None),
            P("sp", None, None),
            P("sp", None, None),
            P(None, "tp"),
            P(None, "tp"),
            P("tp", None),
        ),
        out_specs=P(("sp", "tp"), None),
        check_vma=False,
    )
```
